512 devices in a mesh: sp: 64 (over z, y), fs: 4 (over x), tp: 2 (over core).
Axes of the slice: x: 4, y: 8, z: 8, core: 2. Of those that a mesh axis runs over, the one named last changes fastest.
Arguments:
- tokens: bfloat16 [4, 32768, 2048], P('fs', ('sp', 'tp')), may hold values from -6 to 6
- norm_gain: float32 [2048], replicated, may hold values from 0.1 to 1.9
- query_weight: bfloat16 [2048, 1024], P('sp', 'tp'), may hold values from -20 to 20
- key_matrix: bfloat16 [2048, 256], P('sp', 'tp'), may hold values from -0.125 to 0.125
- value_matrix: bfloat16 [2048, 256], P('sp', 'tp'), may hold values from -0.125 to 0.125
- pool_in_weight: bfloat16 [2048, 1024], P('sp', 'tp'), may hold values from -0.125 to 0.125
- head_sink_logit: float32 [16], replicated, may hold values from 2 to 6
- pool_mix: bfloat16 [4, 256, 256], replicated, may hold values from -0.375 to 0.375
- pool_gain: float32 [1024], replicated, may hold values from 0.1 to 1.9
- attn_out_weight: bfloat16 [1024, 2048], P('tp', 'sp'), may hold values from -1 to 1
- pool_out_weight: bfloat16 [1024, 2048], P('tp', 'sp'), may hold values from -0.125 to 0.125
Outputs:
- mixed: bfloat16 [4, 32768, 2048], P('fs', ('sp', 'tp'))
- row_log_weight_sum: float32 [4, 16, 32768], P('fs', 'tp', 'sp')
The draws below stay inside these ranges and needn't reach their ends.
All inputs are finite; a program needn't handle non-finite values.
Results may differ from the reference program's by a relative error of at most 0.0095.
The reference program's roundings to bfloat16 on the way count: a program that leaves them out, or rounds other values in their place, can miss the bound.
Values may be sent and summed in bfloat16 or wider, within the bound.
A program may use at most 64 MiB of HBM per device.

```python
import jax
import jax.numpy as jnp
from jax import lax

MODEL_WIDTH = 2048
HEAD_SIZE = 64
QUERY_HEADS = 16
KEY_VALUE_HEADS = 4
WINDOW = 128
POOL_GROUPS = 4
POOL_CH = 256
LEN = 32768
SEQS = 4


def draw_query_weight(key, part):
    base = jax.random.normal(jax.random.fold_in(key, 11), (MODEL_WIDTH, QUERY_HEADS * HEAD_SIZE), jnp.float32)
    base = jnp.clip(base, -6.0, 6.0) * MODEL_WIDTH ** (-0.5)
    return jnp.clip(base, -20.0, 20.0).astype(jnp.bfloat16)


def levels(rng, shape, shards, least, high):
    def one(axis_at, parts):
        heights = jax.random.uniform(jax.random.fold_in(jax.random.fold_in(rng, 6), axis_at), (parts,), jnp.float32, least / len(shards), high / len(shards))
        return jnp.repeat(jnp.exp(heights), shape[axis_at] // parts).reshape((-1,) + (1,) * (len(shape) - axis_at - 1))

    level = one(*shards[0])
    for cut in shards[1:]:
        level = level * one(*cut)
    return level


def bell_draw(rng, extent, deviation, reach, cuts=(), kind=jnp.bfloat16):
    values = deviation * jax.random.normal(rng, extent, jnp.float32)
    if cuts:
        values = values * levels(rng, extent, cuts, -0.22, 0.18)
    return jnp.clip(values, -reach, reach).astype(kind)


def setup_inputs(seed: int = 0) -> dict:
    seeds = jax.random.split(jax.random.key(seed), 12)
    return {
        "tokens": bell_draw(seeds[0], (SEQS, LEN, MODEL_WIDTH), 1.0, 6.0, ((0, 4), (1, 128))),
        "norm_gain": jnp.clip(1.0 + 0.18 * jax.random.normal(seeds[1], (MODEL_WIDTH,), jnp.float32), 0.1, 1.9),
        "query_weight": draw_query_weight(jax.random.fold_in(seeds[11], 71), 0),
        "key_matrix": bell_draw(seeds[3], (MODEL_WIDTH, KEY_VALUE_HEADS * HEAD_SIZE), MODEL_WIDTH ** -0.5, 0.125, ((0, 64), (1, 2))),
        "value_matrix": bell_draw(seeds[4], (MODEL_WIDTH, KEY_VALUE_HEADS * HEAD_SIZE), MODEL_WIDTH ** -0.5, 0.125, ((0, 64), (1, 2))),
        "pool_in_weight": bell_draw(seeds[5], (MODEL_WIDTH, POOL_GROUPS * POOL_CH), MODEL_WIDTH ** -0.5, 0.125, ((0, 64), (1, 2))),
        "head_sink_logit": jnp.clip(jax.random.uniform(seeds[6], (QUERY_HEADS,), jnp.float32, 2.0, 6.0), 2.0, 6.0),
        "pool_mix": bell_draw(seeds[7], (POOL_GROUPS, POOL_CH, POOL_CH), POOL_CH ** -0.5, 0.375),
        "pool_gain": jnp.clip(1.0 + 0.18 * jax.random.normal(seeds[8], (POOL_GROUPS * POOL_CH,), jnp.float32), 0.1, 1.9),
        "attn_out_weight": bell_draw(seeds[9], (QUERY_HEADS * HEAD_SIZE, MODEL_WIDTH), (QUERY_HEADS * HEAD_SIZE // 32) ** -0.5, 1.0, ((0, 2), (1, 64))),
        "pool_out_weight": bell_draw(seeds[10], (POOL_GROUPS * POOL_CH, MODEL_WIDTH), (QUERY_HEADS * HEAD_SIZE + POOL_GROUPS * POOL_CH) ** -0.5, 0.125, ((0, 2), (1, 64))),
    }


EPSILON = 1e-06
POOL_SPANS = (2, 4, 8, 16)

def windowed_attend(query_rows, key_rows, value_rows, sinks, kv_heads, group):
    rows = query_rows.shape[0]
    blocks = rows // WINDOW
    width = key_rows.shape[1]
    ext_keys = jnp.concatenate([jnp.zeros((WINDOW, width), key_rows.dtype), key_rows], 0)
    ext_values = jnp.concatenate([jnp.zeros((WINDOW, width), value_rows.dtype), value_rows], 0)

    def banded(table):
        return jnp.concatenate([table[:rows].reshape(blocks, WINDOW, width), table[WINDOW:].reshape(blocks, WINDOW, width)], axis=1)
    band_keys = banded(ext_keys).reshape(blocks, 2 * WINDOW, kv_heads, HEAD_SIZE).astype(jnp.float32)
    band_values = banded(ext_values).reshape(blocks, 2 * WINDOW, kv_heads, HEAD_SIZE).astype(jnp.float32)
    query_blocks = query_rows.reshape(blocks, WINDOW, kv_heads, group, HEAD_SIZE).astype(jnp.float32)
    scores = jnp.einsum('bqkgd,bskd->bkgqs', query_blocks, band_keys) * HEAD_SIZE ** (-0.5)
    query_pos = jnp.arange(rows).reshape(blocks, WINDOW, 1)
    key_pos = jnp.arange(blocks).reshape(blocks, 1, 1) * WINDOW - WINDOW + jnp.arange(2 * WINDOW).reshape(1, 1, 2 * WINDOW)
    offset = query_pos - key_pos
    allowed = (offset >= 0) & (offset < WINDOW) & (key_pos >= 0)
    scores = jnp.where(allowed[:, None, None], scores, -jnp.inf)
    sink_grid = sinks.astype(jnp.float32).reshape(1, kv_heads, group, 1, 1)
    top = jnp.maximum(lax.optimization_barrier(jnp.max(scores, axis=-1, keepdims=True)), sink_grid)
    weights = jnp.exp(scores - top)
    total = lax.optimization_barrier(jnp.sum(weights, axis=-1, keepdims=True)) + jnp.exp(sink_grid - top)
    probs = (weights / total).astype(jnp.bfloat16).astype(jnp.float32)
    mixed = jnp.einsum('bkgqs,bskd->bqkgd', probs, band_values).astype(jnp.bfloat16)
    row_log_weight_sum = (top + jnp.log(total))[..., 0]
    return (mixed.reshape(rows, kv_heads * group * HEAD_SIZE), row_log_weight_sum.transpose(1, 2, 0, 3).reshape(kv_heads * group, rows))

def pool_branch(pool_input, pool_mix, pool_gain):
    rows = pool_input.shape[0]
    pool_reach = max(POOL_SPANS)
    padded = jnp.concatenate([jnp.zeros((pool_reach, pool_input.shape[1]), jnp.float32), pool_input.astype(jnp.float32)], 0)
    position = jnp.arange(rows).reshape(rows, 1)
    pieces = []
    for index, span in enumerate(POOL_SPANS):
        columns = padded[:, index * POOL_CH:(index + 1) * POOL_CH]
        trailing = jnp.zeros((rows, POOL_CH), jnp.float32)
        for lag in range(span):
            trailing = trailing + columns[pool_reach - lag:pool_reach - lag + rows]
        count = jnp.minimum(position + 1, span).astype(jnp.float32)
        pieces.append(trailing / count - columns[pool_reach:])
    centred = jnp.concatenate(pieces, axis=1).astype(jnp.bfloat16)
    grouped = centred.reshape(rows, POOL_GROUPS, POOL_CH).astype(jnp.float32)
    product = jnp.einsum('rgc,gcd->rgd', grouped, pool_mix.astype(jnp.float32)).reshape(rows, POOL_GROUPS * POOL_CH)
    return (product * pool_gain).astype(jnp.bfloat16)

def reference(tokens, norm_gain, query_weight, key_matrix, value_matrix, pool_in_weight, head_sink_logit, pool_mix, pool_gain, attn_out_weight, pool_out_weight):

    def one_sequence(sequence):
        values_f = sequence.astype(jnp.float32)
        scale = lax.rsqrt(lax.optimization_barrier(jnp.mean(values_f * values_f, axis=-1, keepdims=True)) + EPSILON)
        normed = (values_f * scale * norm_gain).astype(jnp.bfloat16)
        query_rows = jnp.dot(normed, query_weight, preferred_element_type=jnp.float32).astype(jnp.bfloat16)
        key_rows = jnp.dot(normed, key_matrix, preferred_element_type=jnp.float32).astype(jnp.bfloat16)
        value_rows = jnp.dot(normed, value_matrix, preferred_element_type=jnp.float32).astype(jnp.bfloat16)
        pool_input = jnp.dot(normed, pool_in_weight, preferred_element_type=jnp.float32).astype(jnp.bfloat16)
        attention_mixer, row_log_weight_sum = windowed_attend(query_rows, key_rows, value_rows, head_sink_logit, KEY_VALUE_HEADS, QUERY_HEADS // KEY_VALUE_HEADS)
        pool_out = pool_branch(pool_input, pool_mix, pool_gain)
        result = jnp.dot(attention_mixer, attn_out_weight, preferred_element_type=jnp.float32) + jnp.dot(pool_out, pool_out_weight, preferred_element_type=jnp.float32)
        return (result.astype(jnp.bfloat16), row_log_weight_sum)
    mixed, row_log_weight_sum = lax.map(one_sequence, tokens)
    return (mixed, row_log_weight_sum)
```

```python
import jax
import jax.numpy as jnp
from jax import lax
from jax.experimental import pallas as pl
from jax.experimental.pallas import tpu as pltpu
from jax.sharding import PartitionSpec as P

RING = 8
SHARD = 32
HEAD = 64
WIN = 128
POOL_CH = 256
EPSILON = 1e-06
F32 = jnp.float32
BF16 = jnp.bfloat16
MESH = pl.DeviceIdType.MESH
SIGN = (1, -1)


def kernel(
    x_hbm, gain, wq, wk, wv, wp, sink, pmix, pgain, wa, wo,
    out, lse,
    zi, yi, zo, yo, xb, nb, accz, accy, qs, kx, vx, px, ma, mp, ob, rb,
    loc_sem, tok_sem, p1s, p1r, bks, bkr, hls, hlr, exs, exr,
):
    R = RING
    half = R // 2
    block = R * SHARD
    rows = xb.shape[0]
    own = rows // 2
    sp = lax.axis_index("sp")
    tp = lax.axis_index("tp")
    z, y = sp // R, sp % R
    mine = pl.multiple_of(tp * own, own)
    theirs = pl.multiple_of((1 - tp) * own, own)
    nq = wq.shape[1]

    def along_y(d):
        return {"sp": z * R + (y + d + R) % R}

    def along_z(d):
        return {"sp": ((z + d + R) % R) * R + y}

    streams = (
        (zi, z, y, along_y, along_z),
        (yi, y, z, along_z, along_y),
        (zo, z, y, along_y, along_z),
        (yo, y, z, along_z, along_y),
    )

    def first(k, d):
        buf, major, minor, peer, _ = streams[k]
        ref = buf.at[major, minor]
        return pltpu.make_async_remote_copy(
            src_ref=ref, dst_ref=ref, send_sem=p1s.at[k, d], recv_sem=p1r.at[k, d],
            device_id=peer(d), device_id_type=MESH,
        )

    def bulk(k, way, s, c):
        buf, major, _, _, peer = streams[k]
        sign = SIGN[way]
        ref = buf.at[(major - sign * (s - 1) + R) % R, pl.ds(c * half, half)]
        return pltpu.make_async_remote_copy(
            src_ref=ref, dst_ref=ref, send_sem=bks.at[k, way, s, c], recv_sem=bkr.at[k, way, s, c],
            device_id=peer(sign), device_id_type=MESH,
        )

    def is_sent(way, s, c):
        return s < half or (s == half and c == way)

    def forward(k, s, c):
        for way in (0, 1):
            if is_sent(way, s, c):
                bulk(k, way, s, c).wait_recv()
                if is_sent(way, s + 1, c):
                    bulk(k, way, s + 1, c).start()

    local = []

    def place(src, dst):
        copy = pltpu.make_async_copy(src, dst, loc_sem.at[len(local)])
        copy.start()
        local.append(copy)

    place(wq, zi.at[z, y, :, pl.ds(0, nq)])
    place(wk, zi.at[z, y, :, pl.ds(nq, wk.shape[1])])
    place(wp, yi.at[y, z, :, pl.ds(0, wp.shape[1])])
    place(wv, yi.at[y, z, :, pl.ds(wp.shape[1], wv.shape[1])])
    place(x_hbm, xb.at[pl.ds(mine, own)])
    place(wa, zo.at[z, y])
    place(wo, yo.at[y, z])

    barrier = pltpu.get_barrier_semaphore()
    peers = [{"tp": 1 - tp}]
    peers += [{"sp": (sp + d + R * R) % (R * R)} for d in (1, -1)]
    for d in range(1, R):
        peers += [along_y(d), along_z(d)]
    for peer in peers:
        pl.semaphore_signal(barrier, inc=1, device_id=peer, device_id_type=MESH)
    pl.semaphore_wait(barrier, len(peers))
    for copy in local:
        copy.wait()

    tokens = pltpu.make_async_remote_copy(
        src_ref=xb.at[pl.ds(mine, own)], dst_ref=xb.at[pl.ds(mine, own)],
        send_sem=tok_sem.at[0], recv_sem=tok_sem.at[1],
        device_id={"tp": 1 - tp}, device_id_type=MESH,
    )
    for d in (1, R - 1, 2, R - 2, 3, R - 3, half):
        if d < R:
            first(0, d).start()
            first(1, d).start()
    tokens.start()

    def norm(start):
        def body(i, carry):
            r = pl.multiple_of(start + i * 32, 32)
            v = xb[pl.ds(r, 32), :].astype(F32)
            scale = lax.rsqrt(jnp.mean(v * v, axis=1, keepdims=True) + EPSILON)
            n = (v * scale * gain[...]).astype(BF16)
            for j in range(R):
                nb[j, pl.ds(r, 32), :] = n[:, j * block : (j + 1) * block]
            return carry

        lax.fori_loop(0, own // 32, body, 0)

    norm(mine)
    px[0:WIN, :] = jnp.zeros((WIN, px.shape[1]), BF16)

    def zero(i, carry):
        r = pl.multiple_of(i * 32, 32)
        accz[pl.ds(r, 32), :] = jnp.zeros((32, accz.shape[1]), F32)
        accy[pl.ds(r, 32), :] = jnp.zeros((32, accy.shape[1]), F32)
        return carry

    lax.fori_loop(0, rows // 32, zero, 0)
    tokens.wait_recv()
    norm(theirs)

    def in_z(b):
        def body(m, carry):
            r = pl.multiple_of(m * own, own)
            w = zi[b].reshape(block, zi.shape[3])
            accz[pl.ds(r, own), :] += jnp.dot(nb[b, pl.ds(r, own), :], w, preferred_element_type=F32)
            return carry

        lax.fori_loop(0, 2, body, 0)

    def in_y(b):
        def body(m, carry):
            r = pl.multiple_of(m * own, own)
            w = yi[:, b].reshape(block, yi.shape[3])
            accy[pl.ds(r, own), :] += jnp.dot(nb[b, pl.ds(r, own), :], w, preferred_element_type=F32)
            return carry

        lax.fori_loop(0, 2, body, 0)

    def own_block(k):
        for d in range(1, R):
            first(k, d).wait_recv()
        for c in (0, 1):
            for way in (0, 1):
                if is_sent(way, 1, c):
                    bulk(k, way, 1, c).start()

    own_block(0)
    own_block(1)
    for d in range(1, R):
        first(2, d).start()
        first(3, d).start()
    in_z(z)
    for s in range(1, half):
        for c in (0, 1):
            forward(0, s, c)
            forward(1, s, c)
        in_z((z + s) % R)
        in_z((z - s + R) % R)
    own_block(2)
    own_block(3)
    for c in (0, 1):
        forward(0, half, c)
        forward(1, half, c)
    in_z((z + half) % R)

    def in_y_all(b, carry):
        in_y(b)
        return carry

    lax.fori_loop(0, R, in_y_all, 0)

    lane = lax.broadcasted_iota(jnp.int32, (32, 128), 1)

    def split(i, carry):
        r = pl.multiple_of(i * 32, 32)
        for p in range(nq // 128):
            t = accz[pl.ds(r, 32), p * 128 : (p + 1) * 128] * (HEAD ** (-0.5))
            turned = pltpu.roll(t, HEAD, 1)
            if p < nq // 256:
                even, odd, keep = t, turned, lane < HEAD
            else:
                even, odd, keep = turned, t, lane >= HEAD
            qs[2 * p, pl.ds(r, 32), :] = jnp.where(keep, even, 0.0).astype(BF16)
            qs[2 * p + 1, pl.ds(r, 32), :] = jnp.where(keep, odd, 0.0).astype(BF16)
        e = pl.multiple_of(WIN + i * 32, 32)
        kx[pl.ds(e, 32), :] = accz[pl.ds(r, 32), nq:].astype(BF16)
        vx[pl.ds(e, 32), :] = accy[pl.ds(r, 32), px.shape[1] :].astype(BF16)
        px[pl.ds(e, 32), :] = accy[pl.ds(r, 32), : px.shape[1]].astype(BF16)
        return carry

    lax.fori_loop(0, rows // 32, split, 0)

    def tail(i, ref, n):
        return pltpu.make_async_remote_copy(
            src_ref=ref.at[pl.ds(WIN + rows - n, n)], dst_ref=ref.at[pl.ds(WIN - n, n)],
            send_sem=hls.at[i], recv_sem=hlr.at[i],
            device_id={"sp": (sp + 1) % (R * R)}, device_id_type=MESH,
        )

    tails = (tail(0, kx, WIN), tail(1, vx, WIN), tail(2, px, 16))

    heads = qs.shape[0]
    group = heads // 2

    def attend(b):
        r = pl.multiple_of(b * WIN, WIN)
        keys = kx[pl.ds(r, 2 * WIN), :]
        values = vx[pl.ds(r, 2 * WIN), :]
        i = lax.broadcasted_iota(jnp.int32, (WIN, 2 * WIN), 0)
        j = lax.broadcasted_iota(jnp.int32, (WIN, 2 * WIN), 1)
        low = jnp.where((sp == 0) & (b == 0), WIN, 0)
        allowed = (j > i) & (j <= i + WIN) & (j >= low)
        lane = lax.broadcasted_iota(jnp.int32, (WIN, 128), 1)
        logs = jnp.zeros((WIN, 128), F32)
        outs = []
        for h in range(heads):
            score = lax.dot_general(
                qs[h, pl.ds(r, WIN), :], keys, (((1,), (1,)), ((), ())), preferred_element_type=F32
            )
            score = jnp.where(allowed, score, -jnp.inf)
            s = sink[tp * heads + h]
            top = jnp.maximum(jnp.max(score, axis=1, keepdims=True), s)
            weight = jnp.exp(score - top)
            total = jnp.sum(weight, axis=1, keepdims=True) + jnp.exp(s - top)
            probs = (weight * (1.0 / total)).astype(BF16)
            outs.append(jnp.dot(probs, values, preferred_element_type=F32))
            logs = jnp.where(lane == h, top + jnp.log(total), logs)
            if h % 2 == 1:
                even, odd = outs
                outs = []
                if h < group:
                    odd = pltpu.roll(odd, HEAD, 1)
                else:
                    even = pltpu.roll(even, HEAD, 1)
                p = h // 2
                ma[pl.ds(r, WIN), p * 128 : (p + 1) * 128] = jnp.where(lane < HEAD, even, odd).astype(BF16)
        lse[:, pl.ds(r, WIN)] = jnp.transpose(logs)[:heads, :]

    def pool(b):
        r = pl.multiple_of(b * WIN, WIN)
        i = lax.broadcasted_iota(jnp.int32, (WIN, 2 * WIN), 0)
        j = lax.broadcasted_iota(jnp.int32, (WIN, 2 * WIN), 1)
        low = jnp.where((sp == 0) & (b == 0), WIN, 0)
        lag = i + WIN - j
        pos = sp * rows + b * WIN + lax.broadcasted_iota(jnp.int32, (WIN, POOL_CH), 0)
        for g in range(px.shape[1] // POOL_CH):
            cols = slice(g * POOL_CH, (g + 1) * POOL_CH)
            span = jnp.where(tp == 0, 2 << g, 8 << g)
            band = jnp.where((lag >= 0) & (lag < span) & (j >= low), 1.0, 0.0).astype(BF16)
            ext = px[pl.ds(r, 2 * WIN), cols]
            trailing = jnp.dot(band, ext, preferred_element_type=F32)
            count = jnp.minimum(pos + 1, span).astype(F32)
            centred = (trailing / count - ext[WIN:].astype(F32)).astype(BF16)
            product = jnp.dot(centred, pmix[tp * 2 + g], preferred_element_type=F32)
            scales = pgain[pl.ds(tp * 2 + g, 1), :]
            mp[pl.ds(r, WIN), cols] = (product * scales).astype(BF16)

    def out_z(n):
        def body(m, carry):
            r = pl.multiple_of(m * own, own)
            w = zo[n].reshape(block, zo.shape[3])
            ob[n, pl.ds(r, own), :] = lax.dot_general(
                ma[pl.ds(r, own), :], w, (((1,), (1,)), ((), ())), preferred_element_type=F32
            )
            return carry

        lax.fori_loop(0, 2, body, 0)

    for t in tails:
        t.start()
    attend(1)
    forward(2, 1, 0)
    forward(3, 1, 0)
    attend(2)
    forward(2, 1, 1)
    forward(3, 1, 1)
    attend(3)
    forward(2, 2, 0)
    forward(3, 2, 0)
    for t in tails:
        t.wait_recv()
    attend(0)
    forward(2, 2, 1)
    forward(3, 2, 1)

    def pool_all(b, carry):
        pool(b)
        return carry

    lax.fori_loop(0, rows // WIN, pool_all, 0)
    for s in range(3, half):
        for c in (0, 1):
            forward(2, s, c)
            forward(3, s, c)
    out_z(z)
    for s in range(1, half):
        out_z((z + s) % R)
        out_z((z - s + R) % R)
    for c in (0, 1):
        forward(2, half, c)
    out_z((z + half) % R)
    for c in (0, 1):
        forward(3, half, c)

    def exchange(n):
        return pltpu.make_async_remote_copy(
            src_ref=ob.at[n, pl.ds(theirs, own)], dst_ref=rb.at[n],
            send_sem=exs.at[n], recv_sem=exr.at[n],
            device_id={"tp": 1 - tp}, device_id_type=MESH,
        )

    def out_y(n, r):
        w = yo[:, n].reshape(block, yo.shape[3])
        ob[n, pl.ds(r, own), :] += lax.dot_general(
            mp[pl.ds(r, own), :], w, (((1,), (1,)), ((), ())), preferred_element_type=F32
        )

    def give(n, carry):
        out_y(n, theirs)
        exchange(n).start()
        return carry

    lax.fori_loop(0, R, give, 0)

    def keep(n, carry):
        out_y(n, mine)
        return carry

    lax.fori_loop(0, R, keep, 0)
    for n in range(R):
        exchange(n).wait_recv()
        out[:, n * block : (n + 1) * block] = (ob[n, pl.ds(mine, own), :] + rb[n]).astype(BF16)

    tokens.wait_send()
    for t in tails:
        t.wait_send()
    for n in range(R):
        exchange(n).wait_send()
    for k in range(4):
        for d in range(1, R):
            first(k, d).wait_send()
        for way in (0, 1):
            for s in range(1, half + 1):
                for c in (0, 1):
                    if is_sent(way, s, c):
                        bulk(k, way, s, c).wait_send()


def local(
    tokens, norm_gain, query_weight, key_matrix, value_matrix, pool_in_weight,
    head_sink_logit, pool_mix, pool_gain, attn_out_weight, pool_out_weight,
):
    R = RING
    own, width = tokens.shape[1:]
    rows = 2 * own
    block = R * SHARD
    nq = query_weight.shape[1]
    nk = key_matrix.shape[1]
    npool = pool_in_weight.shape[1]
    heads = nq // HEAD
    groups = pool_mix.shape[0]
    vmem = pl.BlockSpec(memory_space=pltpu.VMEM)
    smem = pl.BlockSpec(memory_space=pltpu.SMEM)
    anywhere = pl.BlockSpec(memory_space=pl.ANY)
    dma = pltpu.SemaphoreType.DMA
    result, logs = pl.pallas_call(
        kernel,
        name="mixer",
        out_shape=(
            jax.ShapeDtypeStruct((own, width), BF16),
            jax.ShapeDtypeStruct((heads, rows), F32),
        ),
        in_specs=[anywhere, vmem, anywhere, anywhere, anywhere, anywhere, smem, vmem, vmem, anywhere, anywhere],
        out_specs=(vmem, vmem),
        scratch_shapes=[
            pltpu.VMEM((R, R, SHARD, nq + nk), BF16),
            pltpu.VMEM((R, R, SHARD, npool + nk), BF16),
            pltpu.VMEM((R, R, SHARD, attn_out_weight.shape[0]), BF16),
            pltpu.VMEM((R, R, SHARD, pool_out_weight.shape[0]), BF16),
            pltpu.VMEM((rows, width), BF16),
            pltpu.VMEM((R, rows, block), BF16),
            pltpu.VMEM((rows, nq + nk), F32),
            pltpu.VMEM((rows, npool + nk), F32),
            pltpu.VMEM((heads, rows, 128), BF16),
            pltpu.VMEM((WIN + rows, nk), BF16),
            pltpu.VMEM((WIN + rows, nk), BF16),
            pltpu.VMEM((WIN + rows, npool), BF16),
            pltpu.VMEM((rows, nq), BF16),
            pltpu.VMEM((rows, npool), BF16),
            pltpu.VMEM((R, rows, block), F32),
            pltpu.VMEM((R, own, block), F32),
            dma((7,)),
            dma((2,)),
            dma((4, R)),
            dma((4, R)),
            dma((4, 2, R // 2 + 1, 2)),
            dma((4, 2, R // 2 + 1, 2)),
            dma((3,)),
            dma((3,)),
            dma((R,)),
            dma((R,)),
        ],
        compiler_params=pltpu.CompilerParams(
            collective_id=0, has_side_effects=True, vmem_limit_bytes=56 * 1024 * 1024
        ),
    )(
        tokens[0],
        norm_gain[None],
        query_weight,
        key_matrix,
        value_matrix,
        pool_in_weight,
        head_sink_logit,
        pool_mix,
        pool_gain.reshape(groups, POOL_CH),
        attn_out_weight.T,
        pool_out_weight.T,
    )
    return (result[None], logs[None])


def solution(mesh):
    in_specs = (
        P("fs", ("sp", "tp"), None),
        P(),
        P("sp", "tp"),
        P("sp", "tp"),
        P("sp", "tp"),
        P("sp", "tp"),
        P(),
        P(),
        P(),
        P("tp", "sp"),
        P("tp", "sp"),
    )
    out_specs = (P("fs", ("sp", "tp"), None), P("fs", "tp", "sp"))
    return jax.shard_map(local, mesh=mesh, in_specs=in_specs, out_specs=out_specs, check_vma=False)
```

```python
import jax
import jax.numpy as jnp
from jax import lax
from jax.experimental import pallas as pl
from jax.experimental.pallas import tpu as pltpu
from jax.sharding import PartitionSpec as P

RING = 8
CHUNKS = 4
SHARD = 32
HEAD = 64
WIN = 128
POOL_CH = 256
EPSILON = 1e-06
F32 = jnp.float32
BF16 = jnp.bfloat16
MESH = pl.DeviceIdType.MESH
SIGN = (1, -1)


def kernel(
    x_hbm, gain_hbm, wq, wk, wv, wp, sink, pmix_hbm, pgain_hbm, wa, wo,
    out, lse,
    zi, yi, zo, yo, xb, nb, accz, accy, qs, kx, vx, px, ma, mp, ob, rb, stage, gain, pmix, pgain,
    loc_sem, tok_sem, p1s, p1r, bks, bkr, xs, xr, hls, hlr, exs, exr, oss,
):
    R = RING
    NC = CHUNKS
    half = R // 2
    chunk = R // NC
    block = R * SHARD
    rows = xb.shape[0]
    own = rows // 2
    sp = lax.axis_index("sp")
    tp = lax.axis_index("tp")
    fs = lax.axis_index("fs")
    nfs = lax.axis_size("fs")
    par = fs % 2
    z, y = sp // R, sp % R
    mine = pl.multiple_of(tp * own, own)
    theirs = pl.multiple_of((1 - tp) * own, own)
    nq, nk, npool = wq.shape[1], wk.shape[1], wp.shape[1]
    heads = qs.shape[0]
    group = heads // 2
    scope = jax.named_scope

    def along_y(d):
        return {"sp": z * R + (y + d + R) % R}

    def along_z(d):
        return {"sp": ((z + d + R) % R) * R + y}

    streams = (
        (zi, z, y, along_y, along_z, nq // 2, 2 * nk),
        (yi, y, z, along_z, along_y, npool // 4, npool // 2),
        (zo, z, y, along_y, along_z, nq // 4, nq // 2),
        (yo, y, z, along_z, along_y, npool // 4, npool // 2),
    )

    def ring_cols(k):
        side, middle = streams[k][5:]
        return pl.ds(pl.multiple_of(par * side, 128), side + middle)

    def send(ref, send_sem, recv_sem, peer):
        return pltpu.make_async_remote_copy(
            src_ref=ref, dst_ref=ref, send_sem=send_sem, recv_sem=recv_sem,
            device_id=peer, device_id_type=MESH,
        )

    def first(k, d):
        buf, major, minor, peer = streams[k][:4]
        return send(buf.at[major, minor, :, ring_cols(k)], p1s.at[k, d], p1r.at[k, d], peer(d))

    def shard(k, way, s):
        buf, major, minor, peer = streams[k][:4]
        sign = SIGN[way]
        d = s if way == 0 else R - s
        ref = buf.at[major, (minor - sign * (s - 1) + R) % R, :, ring_cols(k)]
        return send(ref, p1s.at[k, d], p1r.at[k, d], peer(sign))

    def shard_is_sent(way, s):
        return s <= half if way == 0 else s < half

    def relay(k, s):
        for way in (0, 1):
            if s > 0 and shard_is_sent(way, s):
                shard(k, way, s).wait_recv()
            if shard_is_sent(way, s + 1):
                shard(k, way, s + 1).start()

    def bulk(k, way, s, c):
        buf, major, _, _, peer = streams[k][:5]
        sign = SIGN[way]
        ref = buf.at[(major - sign * (s - 1) + R) % R, pl.ds(c * chunk, chunk), :, ring_cols(k)]
        return send(ref, bks.at[k, way, s, c], bkr.at[k, way, s, c], peer(sign))

    def is_sent(way, s, c):
        return s < half or (s == half and (c < NC // 2) == (way == 0))

    def cross(k, j, c):
        buf, major = streams[k][:2]
        side, middle = streams[k][5:]
        cols = pl.ds(pl.multiple_of(par * (side + middle), 128), side)
        ref = buf.at[(major + j + R) % R, pl.ds(c * chunk, chunk), :, cols]
        step = 1 if c < NC // 2 else nfs - 1
        return send(ref, xs.at[k, j % R, c], xr.at[k, j % R, c], {"fs": (fs + step) % nfs})

    def crossed(k, j):
        for c in range(NC):
            cross(k, j, c).wait_recv()

    def own_block(k):
        for c in range(NC):
            for way in (0, 1):
                if is_sent(way, 1, c):
                    bulk(k, way, 1, c).start()
            cross(k, 0, c).start()

    def forward(k, s, c):
        for way in (0, 1):
            if is_sent(way, s, c):
                bulk(k, way, s, c).wait_recv()
                if is_sent(way, s + 1, c):
                    bulk(k, way, s + 1, c).start()
                cross(k, -SIGN[way] * s, c).start()

    local = []

    def place(src, dst):
        copy = pltpu.make_async_copy(src, dst, loc_sem.at[len(local)])
        copy.start()
        local.append(copy)

    side = pl.multiple_of(par * (nq // 2), 128)
    place(wq.at[:, pl.ds(side, nq // 2)], zi.at[z, y, :, pl.ds(pl.multiple_of(par * (nq // 2 + 2 * nk), 128), nq // 2)])
    place(wk, zi.at[z, y, :, pl.ds(nq // 2, nk)])
    place(wv, zi.at[z, y, :, pl.ds(nq // 2 + nk, nk)])
    place(wp.at[:, ring_cols(1)], yi.at[y, z, :, ring_cols(1)])
    place(wa.at[:, ring_cols(2)], zo.at[z, y, :, ring_cols(2)])
    place(wo.at[:, ring_cols(3)], yo.at[y, z, :, ring_cols(3)])
    place(x_hbm, xb.at[pl.ds(mine, own)])
    place(gain_hbm, gain)
    place(pmix_hbm.at[pl.ds(tp * pmix.shape[0], pmix.shape[0])], pmix)
    place(pgain_hbm.at[:, pl.ds(pl.multiple_of(tp * npool, 128), npool)], pgain)

    barrier = pltpu.get_barrier_semaphore()
    peers = [{"tp": 1 - tp}]
    peers += [{"sp": (sp + d + R * R) % (R * R)} for d in (1, -1)]
    peers += [{"fs": (fs + d) % nfs} for d in (1, nfs - 1)]
    for d in range(1, R):
        peers += [along_y(d), along_z(d)]
    for peer in peers:
        pl.semaphore_signal(barrier, inc=1, device_id=peer, device_id_type=MESH)
    with scope("barrier"):
        pl.semaphore_wait(barrier, len(peers))
        for copy in local:
            copy.wait()

    tokens = send(xb.at[pl.ds(mine, own)], tok_sem.at[0], tok_sem.at[1], {"tp": 1 - tp})
    for d in range(half, 0, -1):
        for e in sorted({d, R - d}):
            first(0, e).start()
            first(1, e).start()
    tokens.start()

    def norm(start):
        def body(i, carry):
            r = pl.multiple_of(start + i * 32, 32)
            v = xb[pl.ds(r, 32), :].astype(F32)
            scale = lax.rsqrt(jnp.mean(v * v, axis=1, keepdims=True) + EPSILON)
            n = (v * scale * gain[...]).astype(BF16)
            for j in range(R):
                nb[j, pl.ds(r, 32), :] = n[:, j * block : (j + 1) * block]
            return carry

        lax.fori_loop(0, own // 32, body, 0)

    def zero(i, carry):
        r = pl.multiple_of(i * 32, 32)
        accz[pl.ds(r, 32), :] = jnp.zeros((32, accz.shape[1]), F32)
        accy[pl.ds(r, 32), :] = jnp.zeros((32, accy.shape[1]), F32)
        return carry

    with scope("norm"):
        norm(mine)
        px[0:WIN, :] = jnp.zeros((WIN, npool), BF16)
        lax.fori_loop(0, rows // 32, zero, 0)
        tokens.wait_recv()
        norm(theirs)

    def in_z(j):
        b = (z + j + R) % R

        def body(m, carry):
            r = pl.multiple_of(m * own, own)
            w = zi[b].reshape(block, zi.shape[3])
            accz[pl.ds(r, own), :] += jnp.dot(nb[b, pl.ds(r, own), :], w, preferred_element_type=F32)
            return carry

        with scope("in_z"):
            crossed(0, j)
            lax.fori_loop(0, 2, body, 0)

    def in_y(first_b, n):
        def body(m, carry):
            b = first_b + m // 2
            r = pl.multiple_of((m % 2) * own, own)
            w = yi[:, b].reshape(block, yi.shape[3])
            accy[pl.ds(r, own), :] += jnp.dot(nb[b, pl.ds(r, own), :], w, preferred_element_type=F32)
            return carry

        with scope("in_y"):
            lax.fori_loop(0, 2 * n, body, 0)

    with scope("first"):
        for k in (0, 1):
            for d in range(1, R):
                first(k, d).wait_recv()
            own_block(k)
    relay(2, 0)
    relay(3, 0)

    steps = [(s, c) for s in range(1, half + 1) for c in range(NC)]
    relays = iter(range(1, half + 1))
    order = [0] + [j for s in range(1, half) for j in (s, -s)] + [half]
    ready = iter(order)
    for i, (s, c) in enumerate(steps):
        with scope("in_ring"):
            forward(0, s, c)
            forward(1, s, c)
        if i % 2 == 1:
            r = next(relays, None)
            if r is not None:
                with scope("relay"):
                    relay(2, r)
                    relay(3, r)
        if (s, c) == (half - 1, NC - 1):
            own_block(2)
            own_block(3)
        if s > 1 and c in (1, 2) and s <= half or (s, c) == (1, 2):
            in_z(next(ready))

    def split_z(i, carry):
        r = pl.multiple_of(i * 32, 32)
        lane = lax.broadcasted_iota(jnp.int32, (32, 128), 1)
        for p in range(heads // 2):
            at = p * 128 if p < heads // 4 else p * 128 + 2 * nk
            t = accz[pl.ds(r, 32), at : at + 128] * (HEAD ** (-0.5))
            turned = pltpu.roll(t, HEAD, 1)
            if p < heads // 4:
                even, odd, keep = t, turned, lane < HEAD
            else:
                even, odd, keep = turned, t, lane >= HEAD
            qs[2 * p, pl.ds(r, 32), :] = jnp.where(keep, even, 0.0).astype(BF16)
            qs[2 * p + 1, pl.ds(r, 32), :] = jnp.where(keep, odd, 0.0).astype(BF16)
        e = pl.multiple_of(WIN + i * 32, 32)
        kx[pl.ds(e, 32), :] = accz[pl.ds(r, 32), nq // 2 : nq // 2 + nk].astype(BF16)
        vx[pl.ds(e, 32), :] = accz[pl.ds(r, 32), nq // 2 + nk : nq // 2 + 2 * nk].astype(BF16)
        return carry

    def split_y(i, carry):
        r = pl.multiple_of(i * 32, 32)
        e = pl.multiple_of(WIN + i * 32, 32)
        px[pl.ds(e, 32), :] = accy[pl.ds(r, 32), :].astype(BF16)
        return carry

    def tail(i, ref, n):
        return pltpu.make_async_remote_copy(
            src_ref=ref.at[pl.ds(WIN + rows - n, n)], dst_ref=ref.at[pl.ds(WIN - n, n)],
            send_sem=hls.at[i], recv_sem=hlr.at[i],
            device_id={"sp": (sp + 1) % (R * R)}, device_id_type=MESH,
        )

    tails = (tail(0, kx, WIN), tail(1, vx, WIN), tail(2, px, 16))

    def attend(b):
        r = pl.multiple_of(b * WIN, WIN)
        keys = kx[pl.ds(r, 2 * WIN), :]
        values = vx[pl.ds(r, 2 * WIN), :]
        i = lax.broadcasted_iota(jnp.int32, (WIN, 2 * WIN), 0)
        j = lax.broadcasted_iota(jnp.int32, (WIN, 2 * WIN), 1)
        low = jnp.where((sp == 0) & (b == 0), WIN, 0)
        allowed = (j > i) & (j <= i + WIN) & (j >= low)
        lane = lax.broadcasted_iota(jnp.int32, (WIN, 128), 1)
        logs = jnp.zeros((WIN, 128), F32)
        outs = []
        for h in range(heads):
            score = lax.dot_general(
                qs[h, pl.ds(r, WIN), :], keys, (((1,), (1,)), ((), ())), preferred_element_type=F32
            )
            score = jnp.where(allowed, score, -jnp.inf)
            s = sink[tp * heads + h]
            top = jnp.maximum(jnp.max(score, axis=1, keepdims=True), s)
            weight = jnp.exp(score - top)
            total = jnp.sum(weight, axis=1, keepdims=True) + jnp.exp(s - top)
            probs = (weight * (1.0 / total)).astype(BF16)
            outs.append(jnp.dot(probs, values, preferred_element_type=F32))
            logs = jnp.where(lane == h, top + jnp.log(total), logs)
            if h % 2 == 1:
                even, odd = outs
                outs = []
                if h < group:
                    odd = pltpu.roll(odd, HEAD, 1)
                else:
                    even = pltpu.roll(even, HEAD, 1)
                p = h // 2
                ma[pl.ds(r, WIN), p * 128 : (p + 1) * 128] = jnp.where(lane < HEAD, even, odd).astype(BF16)
        lse[:, pl.ds(r, WIN)] = jnp.transpose(logs)[:heads, :]

    def attend_at(b):
        with scope("attend"):
            attend(b)

    def pool(b):
        r = pl.multiple_of(b * WIN, WIN)
        i = lax.broadcasted_iota(jnp.int32, (WIN, 2 * WIN), 0)
        j = lax.broadcasted_iota(jnp.int32, (WIN, 2 * WIN), 1)
        low = jnp.where((sp == 0) & (b == 0), WIN, 0)
        lag = i + WIN - j
        pos = sp * rows + b * WIN + lax.broadcasted_iota(jnp.int32, (WIN, POOL_CH), 0)
        for g in range(npool // POOL_CH):
            cols = slice(g * POOL_CH, (g + 1) * POOL_CH)
            span = jnp.where(tp == 0, 2 << g, 8 << g)
            band = jnp.where((lag >= 0) & (lag < span) & (j >= low), 1.0, 0.0).astype(BF16)
            ext = px[pl.ds(r, 2 * WIN), cols]
            trailing = jnp.dot(band, ext, preferred_element_type=F32)
            count = jnp.minimum(pos + 1, span).astype(F32)
            centred = (trailing / count - ext[WIN:].astype(F32)).astype(BF16)
            product = jnp.dot(centred, pmix[g], preferred_element_type=F32)
            mp[pl.ds(r, WIN), cols] = (product * pgain[:, cols]).astype(BF16)

    def pool_all(b, carry):
        pool(b)
        return carry

    def out_z(j):
        n = (z + j + R) % R

        def body(m, carry):
            r = pl.multiple_of(m * own, own)
            w = zo[n].reshape(block, zo.shape[3])
            ob[n, pl.ds(r, own), :] = lax.dot_general(
                ma[pl.ds(r, own), :], w, (((1,), (1,)), ((), ())), preferred_element_type=F32
            )
            return carry

        with scope("out_z"):
            crossed(2, j)
            lax.fori_loop(0, 2, body, 0)

    def split_all():
        with scope("split_z"):
            lax.fori_loop(0, rows // 32, split_z, 0)
            tails[0].start()
            tails[1].start()

    def in_y_ready():
        with scope("in_y_wait"):
            for j in order:
                crossed(1, j)

    def split_pool():
        with scope("split_y"):
            lax.fori_loop(0, rows // 32, split_y, 0)
            tails[2].start()

    def pool_now():
        with scope("tail_wait"):
            tails[0].wait_recv()
            tails[1].wait_recv()
            tails[2].wait_recv()
        with scope("pool"):
            lax.fori_loop(0, rows // WIN, pool_all, 0)

    pieces = [lambda j=j: in_z(j) for j in ready]
    pieces += [split_all, in_y_ready]
    pieces += [lambda b=b: in_y(b, 2) for b in range(0, R, 2)]
    pieces += [split_pool]
    pieces += [lambda b=b: attend_at(b) for b in range(1, rows // WIN)]
    pieces += [pool_now, lambda: attend_at(0)]
    late = [lambda j=j: out_z(j) for j in order]
    for i, (s, c) in enumerate(steps):
        if i < len(pieces):
            pieces[i]()
        with scope("out_ring"):
            forward(2, s, c)
            forward(3, s, c)
        if s == half and late:
            late.pop(0)()
    for piece in pieces[len(steps) :] + late:
        piece()

    def exchange(n):
        return pltpu.make_async_remote_copy(
            src_ref=ob.at[n, pl.ds(theirs, own)], dst_ref=rb.at[n],
            send_sem=exs.at[n], recv_sem=exr.at[n],
            device_id={"tp": 1 - tp}, device_id_type=MESH,
        )

    def result(n):
        cols = pl.ds(pl.multiple_of(n * block, 128), block)
        return pltpu.make_async_copy(stage.at[n], out.at[:, cols], oss.at[n])

    def out_y(n, r):
        w = yo[:, n].reshape(block, yo.shape[3])
        ob[n, pl.ds(r, own), :] += lax.dot_general(
            mp[pl.ds(r, own), :], w, (((1,), (1,)), ((), ())), preferred_element_type=F32
        )

    def give(n, carry):
        out_y(n, theirs)
        exchange(n).start()
        return carry

    def keep(n, carry):
        out_y(n, mine)
        exchange(n).wait_recv()
        stage[n] = (ob[n, pl.ds(mine, own), :] + rb[n]).astype(BF16)
        result(n).start()
        return carry

    with scope("out_y_wait"):
        for j in order:
            crossed(3, j)
    with scope("give"):
        lax.fori_loop(0, R, give, 0)
    with scope("keep"):
        lax.fori_loop(0, R, keep, 0)

    with scope("drain"):
        tokens.wait_send()
        for t in tails:
            t.wait_send()
        for k in range(4):
            for d in range(1, R):
                first(k, d).wait_send()
            for s, c in steps:
                for way in (0, 1):
                    if is_sent(way, s, c):
                        bulk(k, way, s, c).wait_send()
            for j in order:
                for c in range(NC):
                    cross(k, j, c).wait_send()
        for n in range(R):
            exchange(n).wait_send()
            result(n).wait()


def local(
    tokens, norm_gain, query_weight, key_matrix, value_matrix, pool_in_weight,
    head_sink_logit, pool_mix, pool_gain, attn_out_weight, pool_out_weight,
):
    R = RING
    own, width = tokens.shape[1:]
    rows = 2 * own
    block = R * SHARD
    nq = query_weight.shape[1]
    nk = key_matrix.shape[1]
    npool = pool_in_weight.shape[1]
    heads = nq // HEAD
    groups = pool_mix.shape[0]
    vmem = pl.BlockSpec(memory_space=pltpu.VMEM)
    smem = pl.BlockSpec(memory_space=pltpu.SMEM)
    anywhere = pl.BlockSpec(memory_space=pl.ANY)
    dma = pltpu.SemaphoreType.DMA
    result, logs = pl.pallas_call(
        kernel,
        name="mixer",
        out_shape=(
            jax.ShapeDtypeStruct((own, width), BF16),
            jax.ShapeDtypeStruct((heads, rows), F32),
        ),
        in_specs=[anywhere] * 6 + [smem] + [anywhere] * 4,
        out_specs=(anywhere, vmem),
        scratch_shapes=[
            pltpu.VMEM((R, R, SHARD, nq + 2 * nk), BF16),
            pltpu.VMEM((R, R, SHARD, npool), BF16),
            pltpu.VMEM((R, R, SHARD, attn_out_weight.shape[0]), BF16),
            pltpu.VMEM((R, R, SHARD, pool_out_weight.shape[0]), BF16),
            pltpu.VMEM((rows, width), BF16),
            pltpu.VMEM((R, rows, block), BF16),
            pltpu.VMEM((rows, nq + 2 * nk), F32),
            pltpu.VMEM((rows, npool), F32),
            pltpu.VMEM((heads, rows, 128), BF16),
            pltpu.VMEM((WIN + rows, nk), BF16),
            pltpu.VMEM((WIN + rows, nk), BF16),
            pltpu.VMEM((WIN + rows, npool), BF16),
            pltpu.VMEM((rows, nq), BF16),
            pltpu.VMEM((rows, npool), BF16),
            pltpu.VMEM((R, rows, block), F32),
            pltpu.VMEM((R, own, block), F32),
            pltpu.VMEM((R, own, block), BF16),
            pltpu.VMEM((1, width), F32),
            pltpu.VMEM((groups // 2, POOL_CH, POOL_CH), BF16),
            pltpu.VMEM((1, npool), F32),
            dma((10,)),
            dma((2,)),
            dma((4, R)),
            dma((4, R)),
            dma((4, 2, R // 2 + 1, CHUNKS)),
            dma((4, 2, R // 2 + 1, CHUNKS)),
            dma((4, R, CHUNKS)),
            dma((4, R, CHUNKS)),
            dma((3,)),
            dma((3,)),
            dma((R,)),
            dma((R,)),
            dma((R,)),
        ],
        compiler_params=pltpu.CompilerParams(
            collective_id=0, has_side_effects=True, vmem_limit_bytes=56 * 1024 * 1024
        ),
    )(
        tokens[0],
        norm_gain[None],
        query_weight,
        key_matrix,
        value_matrix,
        pool_in_weight,
        head_sink_logit,
        pool_mix,
        pool_gain[None],
        attn_out_weight.T,
        pool_out_weight.T,
    )
    return (result[None], logs[None])


def solution(mesh):
    in_specs = (
        P("fs", ("sp", "tp"), None),
        P(),
        P("sp", "tp"),
        P("sp", "tp"),
        P("sp", "tp"),
        P("sp", "tp"),
        P(),
        P(),
        P(),
        P("tp", "sp"),
        P("tp", "sp"),
    )
    out_specs = (P("fs", ("sp", "tp"), None), P("fs", "tp", "sp"))
    return jax.shard_map(local, mesh=mesh, in_specs=in_specs, out_specs=out_specs, check_vma=False)
```

```python
import jax
import jax.numpy as jnp
from jax import lax
from jax.experimental import pallas as pl
from jax.experimental.pallas import tpu as pltpu
from jax.sharding import PartitionSpec as P

RING = 8
CHUNKS = 4
SHARD = 32
HEAD = 64
WIN = 128
POOL_CH = 256
EPSILON = 1e-06
F32 = jnp.float32
BF16 = jnp.bfloat16
MESH = pl.DeviceIdType.MESH
SIGN = (1, -1)


def kernel(
    x_hbm, gain_hbm, wq, wk, wv, wp, sink_hbm, pmix_hbm, pgain_hbm, wa, wo,
    out, lse,
    zi, yi, zo, yo, xb, nb, accz, accy, qs, kx, vx, px, ma, mp, ob, rb, sink, gain, pmix, pgain,
    loc_sem, tok_sem, sent, p1r, bkr, xr, hls, hlr, exs, exr,
):
    R = RING
    NC = CHUNKS
    half = R // 2
    chunk = R // NC
    block = R * SHARD
    rows = xb.shape[0]
    own = rows // 2
    sp = lax.axis_index("sp")
    tp = lax.axis_index("tp")
    fs = lax.axis_index("fs")
    nfs = lax.axis_size("fs")
    par = fs % 2
    z, y = sp // R, sp % R
    mine = pl.multiple_of(tp * own, own)
    theirs = pl.multiple_of((1 - tp) * own, own)
    nq, nk, npool = wq.shape[1], wk.shape[1], wp.shape[1]
    heads = nq // HEAD
    scope = jax.named_scope

    def along_y(d):
        return {"sp": z * R + (y + d + R) % R}

    def along_z(d):
        return {"sp": ((z + d + R) % R) * R + y}

    a, b = z + tp * (y - z), y + tp * (z - y)
    stride_a, stride_b = R - tp * (R - 1), 1 + tp * (R - 1)

    def along_a(d):
        return {"sp": (a + d + R) % R * stride_a + b * stride_b}

    def along_b(d):
        return {"sp": a * stride_a + (b + d + R) % R * stride_b}

    streams = (
        (zi, a, b, along_b, along_a, nq // 2, 2 * nk),
        (yi, b, a, along_a, along_b, npool // 4, npool // 2),
        (zo, z, y, along_y, along_z, nq // 4, nq // 2),
        (yo, y, z, along_z, along_y, npool // 4, npool // 2),
    )

    def ring_cols(k):
        side, middle = streams[k][5:]
        return pl.ds(pl.multiple_of(par * side, 128), side + middle)

    def send(ref, send_sem, recv_sem, peer):
        return pltpu.make_async_remote_copy(
            src_ref=ref, dst_ref=ref, send_sem=send_sem, recv_sem=recv_sem,
            device_id=peer, device_id_type=MESH,
        )

    def first(k, d):
        buf, major, minor, peer = streams[k][:4]
        return send(buf.at[major, minor, :, ring_cols(k)], sent.at[k, 2], p1r.at[k, d], peer(d))

    def second(k, d, hop):
        buf, major, minor, peer = streams[k][:4]
        ref = buf.at[major, (minor - d + R) % R, :, ring_cols(k)]
        return send(ref, sent.at[k, 2], p1r.at[k, (d + hop) % R], peer(hop))

    FURTHER = ((2, 1), (R - 2, -1), (2, 2))

    def piece_of(k, c):
        start = (streams[k][2] // chunk + c + (c // 2) * (5 - 2 * c)) % NC
        return pl.ds(start * chunk, chunk)

    def bulk(k, way, s, c):
        buf, major, _, _, peer = streams[k][:5]
        sign = SIGN[way]
        ref = buf.at[(major - sign * (s - 1) + R) % R, piece_of(k, c), :, ring_cols(k)]
        return send(ref, sent.at[k, 0], bkr.at[k, way, s, c], peer(sign))

    def is_sent(way, s, c):
        return s < half or (s == half and (c < NC // 2) == (way == 0))

    def side_cols(k, p):
        side, middle = streams[k][5:]
        return pl.ds(pl.multiple_of(p * (side + middle), 128), side)

    def cross(k, j, c):
        buf, major = streams[k][:2]
        ref = buf.at[(major + j + R) % R, piece_of(k, c), :, side_cols(k, par)]
        step = 1 + (nfs - 2) * (c // (NC // 2))
        return send(ref, sent.at[k, 1], xr.at[k, j % R], {"fs": (fs + step) % nfs})

    def crossed(k, j):
        buf, major = streams[k][:2]
        ref = buf.at[(major + j + R) % R, :, :, side_cols(k, 1 - par)]
        send(ref, sent.at[k, 1], xr.at[k, j % R], {"fs": (fs + 1) % nfs}).wait_recv()

    def own_piece(k, c):
        for way in (0, 1):
            bulk(k, way, 1, c).start()

    def forward(k, s, c):
        for way in (0, 1):
            if is_sent(way, s, c):
                bulk(k, way, s, c).wait_recv()
                if is_sent(way, s + 1, c):
                    bulk(k, way, s + 1, c).start()
                cross(k, -SIGN[way] * s, c).start()

    barrier = pltpu.get_barrier_semaphore()
    peers = [{"tp": 1 - tp}]
    peers += [{"sp": (sp + d + R * R) % (R * R)} for d in (1, -1)]
    peers += [{"fs": (fs + d) % nfs} for d in (1, nfs - 1)]
    for d in range(1, R):
        peers += [along_y(d), along_z(d)]
    for peer in peers:
        pl.semaphore_signal(barrier, inc=1, device_id=peer, device_id_type=MESH)

    local = []

    def place(src, dst):
        copy = pltpu.make_async_copy(src, dst, loc_sem.at[len(local)])
        copy.start()
        local.append(copy)

    side = pl.multiple_of(par * (nq // 2), 128)
    place(wq.at[:, pl.ds(side, nq // 2)], zi.at[a, b, :, pl.ds(pl.multiple_of(par * (nq // 2 + 2 * nk), 128), nq // 2)])
    place(wk, zi.at[a, b, :, pl.ds(nq // 2, nk)])
    place(wv, zi.at[a, b, :, pl.ds(nq // 2 + nk, nk)])
    place(wp.at[:, ring_cols(1)], yi.at[b, a, :, ring_cols(1)])
    place(wa.at[:, ring_cols(2)], zo.at[z, y, :, ring_cols(2)])
    place(wo.at[:, ring_cols(3)], yo.at[y, z, :, ring_cols(3)])
    place(x_hbm, xb.at[pl.ds(mine, own)])
    place(gain_hbm, gain)
    place(sink_hbm, sink)
    place(pmix_hbm.at[pl.ds(tp * pmix.shape[0], pmix.shape[0])], pmix)
    place(pgain_hbm.at[:, pl.ds(pl.multiple_of(tp * npool, 128), npool)], pgain)

    with scope("barrier"):
        pl.semaphore_wait(barrier, len(peers))
        for copy in local:
            copy.wait()

    tokens = send(xb.at[pl.ds(mine, own)], tok_sem.at[0], tok_sem.at[1], {"tp": 1 - tp})
    def norm(start):
        def body(i, carry):
            r = pl.multiple_of(start + i * 32, 32)
            v = xb[pl.ds(r, 32), :].astype(F32)
            scale = lax.rsqrt(jnp.mean(v * v, axis=1, keepdims=True) + EPSILON)
            n = v * scale * gain[...]
            for j in range(R):
                nb[tp, j, pl.ds(r, 32), :] = n[:, j * block : (j + 1) * block].astype(BF16)
            lane = lax.broadcasted_iota(jnp.int32, (32, 128), 1) // SHARD
            for j in range(R):
                for g in range(block // 128):
                    t = None
                    for q in range(128 // SHARD):
                        at = (g * (128 // SHARD) + q) * block + j * SHARD
                        a = n[:, at // 128 * 128 : at // 128 * 128 + 128]
                        turn = (q * SHARD - at % 128) % 128
                        a = pltpu.roll(a, turn, 1) if turn else a
                        t = a if t is None else jnp.where(lane == q, a, t)
                    nb[1 - tp, j, pl.ds(r, 32), g * 128 : (g + 1) * 128] = t.astype(BF16)
            return carry

        lax.fori_loop(0, own // 32, body, 0)

    def zero(i, carry):
        r = pl.multiple_of(i * 32, 32)
        accz[pl.ds(r, 32), :] = jnp.zeros((32, accz.shape[1]), F32)
        accy[pl.ds(r, 32), :] = jnp.zeros((32, accy.shape[1]), F32)
        return carry

    def in_z(j):
        n = (a + j + R) % R
        with scope("in_z"):
            crossed(0, j)
            accz[...] += jnp.dot(nb[0, n], zi[n].reshape(block, zi.shape[3]), preferred_element_type=F32)

    def in_y(j):
        n = (b + j + R) % R
        with scope("in_y"):
            crossed(1, j)
            accy[...] += jnp.dot(nb[1, n], yi[n].reshape(block, yi.shape[3]), preferred_element_type=F32)

    for d in (half, 3, R - 3, 2, R - 2, 1, R - 1):
        first(0, d).start()
        first(1, d).start()
    tokens.start()
    with scope("norm"):
        lax.fori_loop(0, rows // 32, zero, 0)
        norm(mine)
    for k in (2, 3):
        for d in (1, R - 1, 2, R - 2):
            first(k, d).start()
    with scope("norm"):
        px[0:WIN, :] = jnp.zeros((WIN, npool), BF16)
        tokens.wait_recv()
        norm(theirs)
    with scope("first"):
        for k in (0, 1):
            for d in range(1, R):
                first(k, d).wait_recv()
        for c in range(NC):
            for k in (0, 1):
                own_piece(k, c)
                cross(k, 0, c).start()

    order = [0] + [j for s in range(1, half) for j in (s, -s)] + [half]
    ready = [lambda j=j, f=f: f(j) for j in order for f in (in_z, in_y)]
    steps = [(s, c) for s in range(1, half) for c in range(NC)]
    steps += [(half, c) for c in (0, 2, 1, 3)]
    for i, (s, c) in enumerate(steps):
        with scope("in_ring"):
            forward(0, s, c)
            forward(1, s, c)
        if i == 1:
            with scope("second"):
                for k in (2, 3):
                    first(k, 2).wait_recv()
                    first(k, R - 2).wait_recv()
                    for d, hop in FURTHER:
                        second(k, d, hop).start()
        if i == 3 * NC - 1:
            with scope("own_out"):
                for k in (2, 3):
                    for d in range(1, R):
                        if d not in (2, R - 2):
                            first(k, d).wait_recv()
                    for n in range(NC):
                        own_piece(k, n)
        if i in (2, 3) or i > NC:
            ready.pop(0)()
    for k in (2, 3):
        for c in range(NC):
            cross(k, 0, c).start()

    def split_z(i, carry):
        r = pl.multiple_of(i * 32, 32)
        e = pl.multiple_of(WIN + i * 32, 32)
        for p in range(heads // 2):
            at = p * 128 if p < heads // 4 else p * 128 + 2 * nk
            q = accz[pl.ds(r, 32), at : at + 128] * (HEAD ** (-0.5))
            qs[pl.ds(r, 32), p * 128 : (p + 1) * 128] = q.astype(BF16)
        for ref, at in ((kx, nq // 2), (vx, nq // 2 + nk)):
            t = accz[pl.ds(r, 32), at : at + nk]
            ref[0, pl.ds(e, 32), :] = t.astype(BF16)
            ref[1, pl.ds(e, 32), :] = pltpu.roll(t, HEAD, 1).astype(BF16)
        return carry

    def split_y(i, carry):
        r = pl.multiple_of(i * 32, 32)
        e = pl.multiple_of(WIN + i * 32, 32)
        px[pl.ds(e, 32), :] = accy[pl.ds(r, 32), :].astype(BF16)
        return carry

    def tail(i, ref, n):
        src, dst = pl.ds(WIN + rows - n, n), pl.ds(WIN - n, n)
        return pltpu.make_async_remote_copy(
            src_ref=ref.at[src] if i == 2 else ref.at[:, src],
            dst_ref=ref.at[dst] if i == 2 else ref.at[:, dst],
            send_sem=hls.at[i], recv_sem=hlr.at[i],
            device_id={"sp": (sp + 1) % (R * R)}, device_id_type=MESH,
        )

    tails = (tail(0, kx, WIN), tail(1, vx, WIN), tail(2, px, 16))

    def attend(b):
        r = pl.multiple_of(b * WIN, WIN)
        i = lax.broadcasted_iota(jnp.int32, (WIN, WIN), 0)
        j = lax.broadcasted_iota(jnp.int32, (WIN, 128), 1)
        older = j > i
        missing = jnp.where((sp == 0) & (b == 0), -jnp.inf, 0.0)
        left = j < HEAD
        halves = (jnp.where(left, 1.0, 0.0).astype(BF16), jnp.where(left, 0.0, 1.0).astype(BF16))
        logs = jnp.zeros((WIN, 128), F32)
        for p in range(heads // 2):
            pair = qs[pl.ds(r, WIN), p * 128 : (p + 1) * 128]
            outs = []
            for odd in (0, 1):
                h = 2 * p + odd
                turned = odd ^ (h // (heads // 2))
                score = lax.dot_general(
                    pair * halves[odd], kx[turned, pl.ds(r, 2 * WIN), :], (((1,), (1,)), ((), ())),
                    preferred_element_type=F32,
                )
                score = jnp.where(older, score[:, :WIN] + missing, score[:, WIN:])
                s = sink[tp * heads + h]
                top = jnp.maximum(jnp.max(score, axis=1, keepdims=True), s)
                weight = jnp.exp(score - top)
                total = jnp.sum(weight, axis=1, keepdims=True) + jnp.exp(s - top)
                probs = weight * (1.0 / total)
                band = jnp.concatenate(
                    [jnp.where(older, probs, 0.0).astype(BF16), jnp.where(older, 0.0, probs).astype(BF16)], axis=1
                )
                outs.append(jnp.dot(band, vx[turned, pl.ds(r, 2 * WIN), :], preferred_element_type=F32))
                logs = jnp.where(j == h, top + jnp.log(total), logs)
            ma[pl.ds(r, WIN), p * 128 : (p + 1) * 128] = jnp.where(left, outs[0], outs[1]).astype(BF16)
        lse[:, pl.ds(r, WIN)] = jnp.transpose(logs)[:heads, :]

    def attend_at(b):
        with scope("attend"):
            attend(b)

    def pool(b):
        r = pl.multiple_of(b * WIN, WIN)
        i = lax.broadcasted_iota(jnp.int32, (WIN, 2 * WIN), 0)
        j = lax.broadcasted_iota(jnp.int32, (WIN, 2 * WIN), 1)
        low = jnp.where((sp == 0) & (b == 0), WIN, 0)
        lag = i + WIN - j
        pos = sp * rows + b * WIN + lax.broadcasted_iota(jnp.int32, (WIN, 1), 0)
        for g in range(npool // POOL_CH):
            cols = slice(g * POOL_CH, (g + 1) * POOL_CH)
            span = jnp.where(tp == 0, 2 << g, 8 << g)
            band = jnp.where((lag >= 0) & (lag < span) & (j >= low), 1.0, 0.0).astype(BF16)
            ext = px[pl.ds(r, 2 * WIN), cols]
            trailing = jnp.dot(band, ext, preferred_element_type=F32)
            count = jnp.minimum(pos + 1, span).astype(F32)
            centred = (trailing * (1.0 / count) - ext[WIN:].astype(F32)).astype(BF16)
            product = jnp.dot(centred, pmix[g], preferred_element_type=F32)
            mp[pl.ds(r, WIN), cols] = (product * pgain[:, cols]).astype(BF16)

    def pool_all(b, carry):
        pool(b)
        return carry

    def out_z(j):
        n = (z + j + R) % R
        with scope("out_z"):
            crossed(2, j)
            w = zo[n].reshape(block, zo.shape[3])
            ob[n] = lax.dot_general(ma[...], w, (((1,), (1,)), ((), ())), preferred_element_type=F32)

    def split_all():
        with scope("split_z"):
            lax.fori_loop(0, rows // 32, split_z, 0)
            tails[0].start()
            tails[1].start()

    def split_pool():
        with scope("split_y"):
            lax.fori_loop(0, rows // 32, split_y, 0)
            tails[2].start()

    def pool_now():
        with scope("tail_wait"):
            for t in tails:
                t.wait_recv()
        with scope("pool"):
            pool(0)

    def out_step(s, c):
        with scope("out_ring"):
            forward(2, s, c)
            forward(3, s, c)

    def attend_step(c, carry):
        attend_at(c + 1)
        out_step(2, c)
        return carry

    def pool_first():
        with scope("pool"):
            lax.fori_loop(1, rows // WIN, pool_all, 0)

    last_z, last_y = ready[-2:]
    before = ready[:-2] + [last_y, split_pool, pool_first, last_z, split_all]
    for c in range(NC):
        while len(before) > NC - 1 - c:
            before.pop(0)()
        out_step(1, c)
    lax.fori_loop(0, rows // WIN - 1, attend_step, 0)
    for c in range(rows // WIN - 1, NC):
        out_step(2, c)
    pool_now()
    out_step(3, 0)
    attend_at(0)
    out_step(3, 1)
    late = [lambda j=j: out_z(j) for j in order]
    for s, c in steps[2 * NC + 2 :]:
        late.pop(0)()
        out_step(s, c)
    for piece in late:
        piece()

    def exchange(n):
        return pltpu.make_async_remote_copy(
            src_ref=ob.at[n, pl.ds(theirs, own)], dst_ref=rb.at[n],
            send_sem=exs.at[0], recv_sem=exr.at[n],
            device_id={"tp": 1 - tp}, device_id_type=MESH,
        )

    def give(n, carry):
        w = yo[:, n].reshape(block, yo.shape[3])
        ob[n] += lax.dot_general(mp[...], w, (((1,), (1,)), ((), ())), preferred_element_type=F32)
        exchange(n).start()
        return carry

    with scope("out_y_wait"):
        for j in order:
            crossed(3, j)
    with scope("give"):
        lax.fori_loop(0, R, give, 0)
    with scope("keep"):
        for n in range(R):
            exchange(n).wait_recv()
            out[:, n * block : (n + 1) * block] = (ob[n, pl.ds(mine, own), :] + rb[n]).astype(BF16)

    with scope("drain"):
        tokens.wait_send()
        for t in tails:
            t.wait_send()
        for k in range(4):
            buf = streams[k][0]
            parts = (
                buf.at[pl.ds(0, R - 1), :, :, ring_cols(k)],
                buf.at[:, :, :, side_cols(k, par)],
                buf.at[0, pl.ds(0, R - 1), :, ring_cols(k)],
            )
            for i, ref in enumerate(parts):
                send(ref, sent.at[k, i], xr.at[k, 0], {"fs": (fs + 1) % nfs}).wait_send()
        ref = ob.at[:, pl.ds(theirs, own)]
        pltpu.make_async_remote_copy(
            src_ref=ref, dst_ref=rb, send_sem=exs.at[0], recv_sem=exr.at[0],
            device_id={"tp": 1 - tp}, device_id_type=MESH,
        ).wait_send()


def local(
    tokens, norm_gain, query_weight, key_matrix, value_matrix, pool_in_weight,
    head_sink_logit, pool_mix, pool_gain, attn_out_weight, pool_out_weight,
):
    R = RING
    own, width = tokens.shape[1:]
    rows = 2 * own
    block = R * SHARD
    nq = query_weight.shape[1]
    nk = key_matrix.shape[1]
    npool = pool_in_weight.shape[1]
    heads = nq // HEAD
    groups = pool_mix.shape[0]
    vmem = pl.BlockSpec(memory_space=pltpu.VMEM)
    anywhere = pl.BlockSpec(memory_space=pl.ANY)
    dma = pltpu.SemaphoreType.DMA
    result, logs = pl.pallas_call(
        kernel,
        name="mixer",
        out_shape=(
            pltpu.VMEM((own, width), BF16),
            pltpu.VMEM((heads, rows), F32),
        ),
        in_specs=[anywhere] * 11,
        out_specs=(vmem, vmem),
        scratch_shapes=[
            pltpu.VMEM((R, R, SHARD, nq + 2 * nk), BF16),
            pltpu.VMEM((R, R, SHARD, npool), BF16),
            pltpu.VMEM((R, R, SHARD, attn_out_weight.shape[0]), BF16),
            pltpu.VMEM((R, R, SHARD, pool_out_weight.shape[0]), BF16),
            pltpu.VMEM((rows, width), BF16),
            pltpu.VMEM((2, R, rows, block), BF16),
            pltpu.VMEM((rows, nq + 2 * nk), F32),
            pltpu.VMEM((rows, npool), F32),
            pltpu.VMEM((rows, nq), BF16),
            pltpu.VMEM((2, WIN + rows, nk), BF16),
            pltpu.VMEM((2, WIN + rows, nk), BF16),
            pltpu.VMEM((WIN + rows, npool), BF16),
            pltpu.VMEM((rows, nq), BF16),
            pltpu.VMEM((rows, npool), BF16),
            pltpu.VMEM((R, rows, block), F32),
            pltpu.VMEM((R, own, block), F32),
            pltpu.SMEM((2 * heads,), F32),
            pltpu.VMEM((1, width), F32),
            pltpu.VMEM((groups // 2, POOL_CH, POOL_CH), BF16),
            pltpu.VMEM((1, npool), F32),
            dma((11,)),
            dma((2,)),
            dma((4, 3)),
            dma((4, R)),
            dma((4, 2, R // 2 + 1, CHUNKS)),
            dma((4, R)),
            dma((3,)),
            dma((3,)),
            dma((1,)),
            dma((R,)),
        ],
        compiler_params=pltpu.CompilerParams(
            collective_id=0, has_side_effects=True, vmem_limit_bytes=56 * 1024 * 1024
        ),
    )(
        tokens[0],
        norm_gain[None],
        query_weight,
        key_matrix,
        value_matrix,
        pool_in_weight,
        head_sink_logit,
        pool_mix,
        pool_gain[None],
        attn_out_weight.T,
        pool_out_weight.T,
    )
    return (result[None], logs[None])


def solution(mesh):
    in_specs = (
        P("fs", ("sp", "tp"), None),
        P(),
        P("sp", "tp"),
        P("sp", "tp"),
        P("sp", "tp"),
        P("sp", "tp"),
        P(),
        P(),
        P(),
        P("tp", "sp"),
        P("tp", "sp"),
    )
    out_specs = (P("fs", ("sp", "tp"), None), P("fs", "tp", "sp"))
    return jax.shard_map(local, mesh=mesh, in_specs=in_specs, out_specs=out_specs, check_vma=False)
```

```python
import jax
import jax.numpy as jnp
from jax import lax
from jax.experimental import pallas as pl
from jax.experimental.pallas import tpu as pltpu
from jax.sharding import PartitionSpec as P

RING = 8
CHUNKS = 4
SHARD = 32
HEAD = 64
WIN = 128
POOL_CH = 256
EPSILON = 1e-06
F32 = jnp.float32
BF16 = jnp.bfloat16
MESH = pl.DeviceIdType.MESH
SIGN = (1, -1)


def kernel(
    x_hbm, gain_hbm, wq, wk, wv, wp, sink_hbm, pmix_hbm, pgain_hbm, wa, wo,
    out, lse,
    zi, yi, zo, yo, xb, nb, accz, accy, qs, kx, vx, px, ma, mp, ob, give_b, rb, sink, gain, pmix, pgain,
    loc_sem, tok_sem, sent, p1r, bkr, xr, hls, hlr, exs, exr,
):
    R = RING
    NC = CHUNKS
    half = R // 2
    chunk = R // NC
    block = R * SHARD
    rows = xb.shape[0]
    own = rows // 2
    sp = lax.axis_index("sp")
    tp = lax.axis_index("tp")
    fs = lax.axis_index("fs")
    nfs = lax.axis_size("fs")
    par = fs % 2
    z, y = sp // R, sp % R
    mine = pl.multiple_of(tp * own, own)
    theirs = pl.multiple_of((1 - tp) * own, own)
    nq, nk, npool = wq.shape[1], wk.shape[1], wp.shape[1]
    heads = nq // HEAD
    scope = jax.named_scope

    def along_y(d):
        return {"sp": z * R + (y + d + R) % R}

    def along_z(d):
        return {"sp": ((z + d + R) % R) * R + y}

    a, b = z + tp * (y - z), y + tp * (z - y)
    stride_a, stride_b = R - tp * (R - 1), 1 + tp * (R - 1)

    def along_a(d):
        return {"sp": (a + d + R) % R * stride_a + b * stride_b}

    def along_b(d):
        return {"sp": a * stride_a + (b + d + R) % R * stride_b}

    streams = (
        (zi, a, b, along_b, along_a, nq // 2, 2 * nk),
        (yi, b, a, along_a, along_b, npool // 4, npool // 2),
        (zo, z, y, along_y, along_z, nq // 4, nq // 2),
        (yo, y, z, along_z, along_y, npool // 4, npool // 2),
    )

    def ring_cols(k):
        side, middle = streams[k][5:]
        return pl.ds(pl.multiple_of(par * side, 128), side + middle)

    def send(ref, send_sem, recv_sem, peer):
        return pltpu.make_async_remote_copy(
            src_ref=ref, dst_ref=ref, send_sem=send_sem, recv_sem=recv_sem,
            device_id=peer, device_id_type=MESH,
        )

    def first(k, d):
        buf, major, minor, peer = streams[k][:4]
        return send(buf.at[major, minor, :, ring_cols(k)], sent.at[k, 2], p1r.at[k, kind(k, d)], peer(d))

    def kind(k, d):
        return int(k > 1 and d % R in (2, R - 2))

    def arrived(k, which, n):
        ref = streams[k][0].at[0, pl.ds(0, n), :, ring_cols(k)]
        send(ref, sent.at[k, 2], p1r.at[k, which], {"fs": (fs + 1) % nfs}).wait_recv()

    def second(k, d, hop):
        buf, major, minor, peer = streams[k][:4]
        ref = buf.at[major, (minor - d + R) % R, :, ring_cols(k)]
        return send(ref, sent.at[k, 2], p1r.at[k, kind(k, d + hop)], peer(hop))

    FURTHER = ((2, 1), (R - 2, -1), (2, 2))

    def piece_of(k, c):
        start = (streams[k][2] // chunk + c + (c // 2) * (5 - 2 * c)) % NC
        return pl.ds(start * chunk, chunk)

    def bulk(k, way, s, c):
        buf, major, _, _, peer = streams[k][:5]
        sign = SIGN[way]
        ref = buf.at[(major - sign * (s - 1) + R) % R, piece_of(k, c), :, ring_cols(k)]
        return send(ref, sent.at[k, 0], bkr.at[k, s - 1, c], peer(sign))

    def is_sent(way, s, c):
        return s < half or (s == half and (c < NC // 2) == (way == 0))

    def side_cols(k, p):
        side, middle = streams[k][5:]
        return pl.ds(pl.multiple_of(p * (side + middle), 128), side)

    def cross(k, j, c):
        buf, major = streams[k][:2]
        ref = buf.at[(major + j + R) % R, piece_of(k, c), :, side_cols(k, par)]
        step = 1 + (nfs - 2) * (c // (NC // 2))
        return send(ref, sent.at[k, 1], xr.at[k, j_abs(j)], {"fs": (fs + step) % nfs})

    def j_abs(j):
        return max(j, -j)

    def crossed(k, j):
        if j >= 0:
            ref = streams[k][0].at[pl.ds(0, 2 if 0 < j < half else 1), :, :, side_cols(k, 1 - par)]
            send(ref, sent.at[k, 1], xr.at[k, j], {"fs": (fs + 1) % nfs}).wait_recv()

    def own_piece(k, c):
        for way in (0, 1):
            bulk(k, way, 1, c).start()

    def forward(k, s, c):
        ways = [way for way in (0, 1) if is_sent(way, s, c)]
        ref = streams[k][0].at[0, pl.ds(0, len(ways) * chunk), :, ring_cols(k)]
        send(ref, sent.at[k, 0], bkr.at[k, s - 1, c], {"fs": (fs + 1) % nfs}).wait_recv()
        for way in ways:
            if is_sent(way, s + 1, c):
                bulk(k, way, s + 1, c).start()
            cross(k, -SIGN[way] * s, c).start()

    barrier = pltpu.get_barrier_semaphore()
    peers = [{"tp": 1 - tp}]
    peers += [{"sp": (sp + d + R * R) % (R * R)} for d in (1, -1)]
    peers += [{"fs": (fs + d) % nfs} for d in (1, nfs - 1)]
    for d in range(1, R):
        peers += [along_y(d), along_z(d)]
    for peer in peers:
        pl.semaphore_signal(barrier, inc=1, device_id=peer, device_id_type=MESH)

    local = []

    def place(src, dst):
        copy = pltpu.make_async_copy(src, dst, loc_sem.at[len(local)])
        copy.start()
        local.append(copy)

    side = pl.multiple_of(par * (nq // 2), 128)
    place(wq.at[:, pl.ds(side, nq // 2)], zi.at[a, b, :, pl.ds(pl.multiple_of(par * (nq // 2 + 2 * nk), 128), nq // 2)])
    place(wk, zi.at[a, b, :, pl.ds(nq // 2, nk)])
    place(wv, zi.at[a, b, :, pl.ds(nq // 2 + nk, nk)])
    place(wp.at[:, ring_cols(1)], yi.at[b, a, :, ring_cols(1)])
    place(x_hbm, xb.at[pl.ds(mine, own)])
    place(gain_hbm, gain)
    place(wa.at[:, ring_cols(2)], zo.at[z, y, :, ring_cols(2)])
    place(wo.at[:, ring_cols(3)], yo.at[y, z, :, ring_cols(3)])
    place(sink_hbm, sink)
    place(pmix_hbm.at[pl.ds(tp * pmix.shape[0], pmix.shape[0])], pmix)
    place(pgain_hbm.at[:, pl.ds(pl.multiple_of(tp * npool, 128), npool)], pgain)

    with scope("barrier"):
        pl.semaphore_wait(barrier, len(peers))
        for copy in local[:4]:
            copy.wait()

    tokens = send(xb.at[pl.ds(mine, own)], tok_sem.at[0], tok_sem.at[1], {"tp": 1 - tp})
    def norm(start):
        def body(i, carry):
            r = pl.multiple_of(start + i * 32, 32)
            v = xb[pl.ds(r, 32), :].astype(F32)
            scale = lax.rsqrt(jnp.mean(v * v, axis=1, keepdims=True) + EPSILON)
            n = v * scale * gain[...]
            for j in range(R):
                nb[tp, j, pl.ds(r, 32), :] = n[:, j * block : (j + 1) * block].astype(BF16)
            lane = lax.broadcasted_iota(jnp.int32, (32, 128), 1) // SHARD
            for j in range(R):
                for g in range(block // 128):
                    t = None
                    for q in range(128 // SHARD):
                        at = (g * (128 // SHARD) + q) * block + j * SHARD
                        a = n[:, at // 128 * 128 : at // 128 * 128 + 128]
                        turn = (q * SHARD - at % 128) % 128
                        a = pltpu.roll(a, turn, 1) if turn else a
                        t = a if t is None else jnp.where(lane == q, a, t)
                    nb[1 - tp, j, pl.ds(r, 32), g * 128 : (g + 1) * 128] = t.astype(BF16)
            return carry

        lax.fori_loop(0, own // 32, body, 0)

    def zero(i, carry):
        r = pl.multiple_of(i * 32, 32)
        accz[pl.ds(r, 32), :] = jnp.zeros((32, accz.shape[1]), F32)
        accy[pl.ds(r, 32), :] = jnp.zeros((32, accy.shape[1]), F32)
        return carry

    def in_z(j):
        n = (a + j + R) % R
        with scope("in_z"):
            crossed(0, j)
            accz[...] += jnp.dot(nb[0, n], zi[n].reshape(block, zi.shape[3]), preferred_element_type=F32)

    def in_y(j):
        n = (b + j + R) % R
        with scope("in_y"):
            crossed(1, j)
            accy[...] += jnp.dot(nb[1, n], yi[n].reshape(block, yi.shape[3]), preferred_element_type=F32)

    for d in (half, 3, R - 3, 2, R - 2, 1, R - 1):
        first(0, d).start()
        first(1, d).start()
    for copy in local[4:]:
        copy.wait()
    tokens.start()
    with scope("norm"):
        lax.fori_loop(0, rows // 32, zero, 0)
        norm(mine)
    for k in (2, 3):
        for d in (1, R - 1, 2, R - 2):
            first(k, d).start()
    with scope("norm"):
        px[0:WIN, :] = jnp.zeros((WIN, npool), BF16)
        tokens.wait_recv()
        norm(theirs)
    with scope("first"):
        for k in (0, 1):
            arrived(k, 0, R - 1)
        for c in range(NC):
            for k in (0, 1):
                own_piece(k, c)
                cross(k, 0, c).start()

    order = [0] + [j for s in range(1, half) for j in (s, -s)] + [half]
    ready = [lambda j=j, f=f: f(j) for j in order for f in (in_z, in_y)]
    steps = [(s, c) for s in range(1, half) for c in range(NC)]
    steps += [(half, c) for c in (0, 2, 1, 3)]
    for i, (s, c) in enumerate(steps):
        with scope("in_ring"):
            forward(0, s, c)
            forward(1, s, c)
        if i == 1:
            with scope("second"):
                for k in (2, 3):
                    arrived(k, 1, 2)
                    for d, hop in FURTHER:
                        second(k, d, hop).start()
        if i == 3 * NC - 1:
            with scope("own_out"):
                for k in (2, 3):
                    arrived(k, 0, R - 3)
                    for n in range(NC):
                        own_piece(k, n)
        for _ in range(4 if i == 3 * NC - 1 else i in (4, 5, 7, 8, 9, 10)):
            ready.pop(0)()
    for k in (2, 3):
        for c in range(NC):
            cross(k, 0, c).start()

    def split_z(i, carry):
        r = pl.multiple_of(i * 128, 128)
        e = pl.multiple_of(WIN + i * 128, 128)
        for p in range(heads // 2):
            at = p * 128 if p < heads // 4 else p * 128 + 2 * nk
            q = accz[pl.ds(r, 128), at : at + 128] * (HEAD ** (-0.5))
            qs[pl.ds(r, 128), p * 128 : (p + 1) * 128] = q.astype(BF16)
        for ref, at in ((kx, nq // 2), (vx, nq // 2 + nk)):
            t = accz[pl.ds(r, 128), at : at + nk]
            ref[0, pl.ds(e, 128), :] = t.astype(BF16)
            ref[1, pl.ds(e, 128), :] = pltpu.roll(t, HEAD, 1).astype(BF16)
        return carry

    def split_y(i, carry):
        r = pl.multiple_of(i * 32, 32)
        e = pl.multiple_of(WIN + i * 32, 32)
        px[pl.ds(e, 32), :] = accy[pl.ds(r, 32), :].astype(BF16)
        return carry

    def tail(i, ref, n):
        src, dst = pl.ds(WIN + rows - n, n), pl.ds(WIN - n, n)
        return pltpu.make_async_remote_copy(
            src_ref=ref.at[src] if i == 2 else ref.at[0, src],
            dst_ref=ref.at[dst] if i == 2 else ref.at[0, dst],
            send_sem=hls.at[i], recv_sem=hlr.at[i],
            device_id={"sp": (sp + 1) % (R * R)}, device_id_type=MESH,
        )

    tails = (tail(0, kx, WIN), tail(1, vx, WIN), tail(2, px, 16))

    def attend(b):
        r = pl.multiple_of(b * WIN, WIN)
        i = lax.broadcasted_iota(jnp.int32, (WIN, WIN), 0)
        j = lax.broadcasted_iota(jnp.int32, (WIN, 128), 1)
        older = j > i
        missing = jnp.where((sp == 0) & (b == 0), -jnp.inf, 0.0)
        left = j < HEAD
        halves = (jnp.where(left, 1.0, 0.0).astype(BF16), jnp.where(left, 0.0, 1.0).astype(BF16))
        logs = jnp.zeros((WIN, 128), F32)
        width = heads // 2
        for g in (0, 1):
            scores = []
            for h in range(g * width, (g + 1) * width):
                pair = qs[pl.ds(r, WIN), h // 2 * 128 : h // 2 * 128 + 128]
                score = lax.dot_general(
                    pair * halves[h % 2], kx[h % 2 ^ g, pl.ds(r, 2 * WIN), :], (((1,), (1,)), ((), ())),
                    preferred_element_type=F32,
                )
                scores.append(jnp.where(older, score[:, :WIN] + missing, score[:, WIN:]))
            sinks = [sink[tp * heads + g * width + n] for n in range(width)]
            tops = [jnp.maximum(jnp.max(v, axis=1, keepdims=True), s) for v, s in zip(scores, sinks)]
            weights = [jnp.exp(v - t) for v, t in zip(scores, tops)]
            totals = [jnp.sum(v, axis=1, keepdims=True) + jnp.exp(s - t) for v, s, t in zip(weights, sinks, tops)]
            outs = []
            for n in range(width):
                probs = weights[n] * (1.0 / totals[n])
                band = jnp.concatenate(
                    [jnp.where(older, probs, 0.0).astype(BF16), jnp.where(older, 0.0, probs).astype(BF16)], axis=1
                )
                outs.append(jnp.dot(band, vx[n % 2 ^ g, pl.ds(r, 2 * WIN), :], preferred_element_type=F32))
            for n in range(width):
                logs = jnp.where(j == g * width + n, tops[n] + jnp.log(totals[n]), logs)
            for n in range(0, width, 2):
                at = (g * width + n) // 2 * 128
                ma[pl.ds(r, WIN), at : at + 128] = jnp.where(left, outs[n], outs[n + 1]).astype(BF16)
        lse[:, pl.ds(r, WIN)] = jnp.transpose(logs)[:heads, :]

    def attend_at(b):
        with scope("attend"):
            attend(b)

    def pool(b):
        r = pl.multiple_of(b * WIN, WIN)
        i = lax.broadcasted_iota(jnp.int32, (WIN, 2 * WIN), 0)
        j = lax.broadcasted_iota(jnp.int32, (WIN, 2 * WIN), 1)
        low = jnp.where((sp == 0) & (b == 0), WIN, 0)
        lag = i + WIN - j
        pos = sp * rows + b * WIN + lax.broadcasted_iota(jnp.int32, (WIN, 1), 0)
        for g in range(npool // POOL_CH):
            cols = slice(g * POOL_CH, (g + 1) * POOL_CH)
            span = jnp.where(tp == 0, 2 << g, 8 << g)
            band = jnp.where((lag >= 0) & (lag < span) & (j >= low), 1.0, 0.0).astype(BF16)
            ext = px[pl.ds(r, 2 * WIN), cols]
            trailing = jnp.dot(band, ext, preferred_element_type=F32)
            count = jnp.minimum(pos + 1, span).astype(F32)
            centred = (trailing * (1.0 / count) - ext[WIN:].astype(F32)).astype(BF16)
            product = jnp.dot(centred, pmix[g], preferred_element_type=F32)
            mp[pl.ds(r, WIN), cols] = (product * pgain[:, cols]).astype(BF16)

    def pool_all(b, carry):
        pool(b)
        return carry

    def out_z(t, carry):
        for n in range(R // 2):
            @pl.when(t == n)
            def _():
                for step in steps[2 * NC + 2 + max(n, 2 * n - 2) :][: 1 if n < 2 else 2]:
                    out_step(*step)
                crossed(2, n + 1)

        for i in (2 * t, 2 * t + 1):
            n = (z + (i + 1) // 2 * (2 * (i % 2) - 1) + R) % R
            w = zo[n].reshape(block, zo.shape[3])
            ob[n] = lax.dot_general(ma[...], w, (((1,), (1,)), ((), ())), preferred_element_type=F32)
        return carry

    def split_all():
        with scope("split_z"):
            lax.fori_loop(0, rows // 128, split_z, 0)
            tails[0].start()
            tails[1].start()

    def split_pool():
        with scope("split_y"):
            lax.fori_loop(0, rows // 32, split_y, 0)
            tails[2].start()

    def pool_now():
        with scope("tail_wait"):
            for t in tails:
                t.wait_recv()
            for ref in (kx, vx):
                ref[1, 0:WIN, :] = pltpu.roll(ref[0, 0:WIN, :].astype(F32), HEAD, 1).astype(BF16)
        with scope("pool"):
            pool(0)

    def out_step(s, c):
        with scope("out_ring"):
            forward(2, s, c)
            forward(3, s, c)

    def attend_step(c, carry):
        attend_at(c + 1)
        for n, step in enumerate(((2, 2), (2, 3), (3, 0))):
            @pl.when(c == n)
            def _():
                out_step(*step)

        return carry

    def pool_first():
        with scope("pool"):
            lax.fori_loop(1, rows // WIN, pool_all, 0)

    last_z, last_y = ready[-2:]
    out_step(1, 0)
    for n, piece in enumerate(ready[:-2]):
        piece()
        if n % 2:
            out_step(1, 1 + n // 2)
    last_y()
    split_pool()
    out_step(1, 3)
    pool_first()
    out_step(2, 0)
    last_z()
    split_all()
    out_step(2, 1)
    lax.fori_loop(0, rows // WIN - 1, attend_step, 0)
    pool_now()
    out_step(3, 1)
    attend_at(0)
    with scope("out_z"):
        crossed(2, 0)
        lax.fori_loop(0, R // 2, out_z, 0)

    def exchange(n):
        return pltpu.make_async_remote_copy(
            src_ref=give_b.at[pl.ds(2 * n, 2)], dst_ref=rb.at[pl.ds(2 * n, 2)],
            send_sem=exs.at[0], recv_sem=exr.at[n],
            device_id={"tp": 1 - tp}, device_id_type=MESH,
        )

    def give(m, carry):
        for n in (2 * m, 2 * m + 1):
            w = yo[:, n].reshape(block, yo.shape[3])
            ob[n] += lax.dot_general(mp[...], w, (((1,), (1,)), ((), ())), preferred_element_type=F32)
            give_b[n] = ob[n, pl.ds(theirs, own), :].astype(BF16)
        exchange(m).start()
        return carry

    with scope("out_y_wait"):
        for j in order:
            crossed(3, j)
    with scope("give"):
        lax.fori_loop(0, R // 2, give, 0)
    with scope("keep"):
        for n in range(R):
            if n % 2 == 0:
                exchange(n // 2).wait_recv()
            out[:, n * block : (n + 1) * block] = (ob[n, pl.ds(mine, own), :] + rb[n].astype(F32)).astype(BF16)

    with scope("drain"):
        tokens.wait_send()
        for t in tails:
            t.wait_send()
        for k in range(4):
            buf = streams[k][0]
            parts = (
                buf.at[pl.ds(0, R - 1), :, :, ring_cols(k)],
                buf.at[:, :, :, side_cols(k, par)],
                buf.at[0, pl.ds(0, R - 1), :, ring_cols(k)],
            )
            for i, ref in enumerate(parts):
                send(ref, sent.at[k, i], xr.at[k, 0], {"fs": (fs + 1) % nfs}).wait_send()
        pltpu.make_async_remote_copy(
            src_ref=give_b, dst_ref=rb, send_sem=exs.at[0], recv_sem=exr.at[0],
            device_id={"tp": 1 - tp}, device_id_type=MESH,
        ).wait_send()


def local(
    tokens, norm_gain, query_weight, key_matrix, value_matrix, pool_in_weight,
    head_sink_logit, pool_mix, pool_gain, attn_out_weight, pool_out_weight,
):
    R = RING
    own, width = tokens.shape[1:]
    rows = 2 * own
    block = R * SHARD
    nq = query_weight.shape[1]
    nk = key_matrix.shape[1]
    npool = pool_in_weight.shape[1]
    heads = nq // HEAD
    groups = pool_mix.shape[0]
    vmem = pl.BlockSpec(memory_space=pltpu.VMEM)
    anywhere = pl.BlockSpec(memory_space=pl.ANY)
    dma = pltpu.SemaphoreType.DMA
    result, logs = pl.pallas_call(
        kernel,
        name="mixer",
        out_shape=(
            pltpu.VMEM((own, width), BF16),
            pltpu.VMEM((heads, rows), F32),
        ),
        in_specs=[anywhere] * 11,
        out_specs=(vmem, vmem),
        scratch_shapes=[
            pltpu.VMEM((R, R, SHARD, nq + 2 * nk), BF16),
            pltpu.VMEM((R, R, SHARD, npool), BF16),
            pltpu.VMEM((R, R, SHARD, attn_out_weight.shape[0]), BF16),
            pltpu.VMEM((R, R, SHARD, pool_out_weight.shape[0]), BF16),
            pltpu.VMEM((rows, width), BF16),
            pltpu.VMEM((2, R, rows, block), BF16),
            pltpu.VMEM((rows, nq + 2 * nk), F32),
            pltpu.VMEM((rows, npool), F32),
            pltpu.VMEM((rows, nq), BF16),
            pltpu.VMEM((2, WIN + rows, nk), BF16),
            pltpu.VMEM((2, WIN + rows, nk), BF16),
            pltpu.VMEM((WIN + rows, npool), BF16),
            pltpu.VMEM((rows, nq), BF16),
            pltpu.VMEM((rows, npool), BF16),
            pltpu.VMEM((R, rows, block), F32),
            pltpu.VMEM((R, own, block), BF16),
            pltpu.VMEM((R, own, block), BF16),
            pltpu.SMEM((2 * heads,), F32),
            pltpu.VMEM((1, width), F32),
            pltpu.VMEM((groups // 2, POOL_CH, POOL_CH), BF16),
            pltpu.VMEM((1, npool), F32),
            dma((11,)),
            dma((2,)),
            dma((4, 3)),
            dma((4, 2)),
            dma((4, R // 2, CHUNKS)),
            dma((4, R // 2 + 1)),
            dma((3,)),
            dma((3,)),
            dma((1,)),
            dma((R // 2,)),
        ],
        compiler_params=pltpu.CompilerParams(
            collective_id=0, has_side_effects=True, vmem_limit_bytes=56 * 1024 * 1024
        ),
    )(
        tokens[0],
        norm_gain[None],
        query_weight,
        key_matrix,
        value_matrix,
        pool_in_weight,
        head_sink_logit,
        pool_mix,
        pool_gain[None],
        attn_out_weight.T,
        pool_out_weight.T,
    )
    return (result[None], logs[None])


def solution(mesh):
    in_specs = (
        P("fs", ("sp", "tp"), None),
        P(),
        P("sp", "tp"),
        P("sp", "tp"),
        P("sp", "tp"),
        P("sp", "tp"),
        P(),
        P(),
        P(),
        P("tp", "sp"),
        P("tp", "sp"),
    )
    out_specs = (P("fs", ("sp", "tp"), None), P("fs", "tp", "sp"))
    return jax.shard_map(local, mesh=mesh, in_specs=in_specs, out_specs=out_specs, check_vma=False)
```

```python
import jax
import jax.numpy as jnp
from jax import lax
from jax.experimental import pallas as pl
from jax.experimental.pallas import tpu as pltpu
from jax.sharding import PartitionSpec as P

RING = 8
CHUNKS = 4
SHARD = 32
HEAD = 64
WIN = 128
POOL_CH = 256
EPSILON = 1e-06
F32 = jnp.float32
BF16 = jnp.bfloat16
MESH = pl.DeviceIdType.MESH
SIGN = (1, -1)
INWARD = (3, 1, 2, 0)


def kernel(
    x_hbm, gain_hbm, wq, wk, wv, wp, sink_hbm, pmix_hbm, pgain_hbm, wa, wo,
    out, lse,
    zi, yi, zo, yo, xb, nb, accz, accy, qs, kx, vx, px, ma, mp, ob, give_b, rb, sink, gain, pmix, pgain,
    loc_sem, tok_sem, sent, p1r, bkr, xr, hls, hlr, exs, exr,
):
    R = RING
    NC = CHUNKS
    half = R // 2
    chunk = R // NC
    block = R * SHARD
    rows = xb.shape[0]
    own = rows // 2
    sp = lax.axis_index("sp")
    tp = lax.axis_index("tp")
    fs = lax.axis_index("fs")
    nfs = lax.axis_size("fs")
    par = fs % 2
    z, y = sp // R, sp % R
    mine = pl.multiple_of(tp * own, own)
    theirs = pl.multiple_of((1 - tp) * own, own)
    nq, nk, npool = wq.shape[1], wk.shape[1], wp.shape[1]
    heads = nq // HEAD
    scope = jax.named_scope

    def along_y(d):
        return {"sp": z * R + (y + d + R) % R}

    def along_z(d):
        return {"sp": ((z + d + R) % R) * R + y}

    a, b = z + tp * (y - z), y + tp * (z - y)
    stride_a, stride_b = R - tp * (R - 1), 1 + tp * (R - 1)

    def along_a(d):
        return {"sp": (a + d + R) % R * stride_a + b * stride_b}

    def along_b(d):
        return {"sp": a * stride_a + (b + d + R) % R * stride_b}

    streams = (
        (zi, a, b, along_b, along_a, nq // 2, 2 * nk),
        (yi, b, a, along_a, along_b, npool // 4, npool // 2),
        (zo, z, y, along_y, along_z, nq // 4, nq // 2),
        (yo, y, z, along_z, along_y, npool // 4, npool // 2),
    )

    def ring_cols(k):
        side, middle = streams[k][5:]
        return pl.ds(pl.multiple_of(par * side, 128), side + middle)

    def send(ref, send_sem, recv_sem, peer):
        return pltpu.make_async_remote_copy(
            src_ref=ref, dst_ref=ref, send_sem=send_sem, recv_sem=recv_sem,
            device_id=peer, device_id_type=MESH,
        )

    def first(k, d):
        buf, major, minor, peer = streams[k][:4]
        return send(buf.at[major, minor, :, ring_cols(k)], sent.at[k, 2], p1r.at[kind(k, d)], peer(d))

    def kind(k, d):
        return 2 * R + 2 * (k - 2) + int(d % R in (2, R - 2)) if k > 1 else k * R + d

    def arrived(k, which, n):
        ref = streams[k][0].at[0, pl.ds(0, n), :, ring_cols(k)]
        send(ref, sent.at[k, 2], p1r.at[2 * R + 2 * (k - 2) + which], {"fs": (fs + 1) % nfs}).wait_recv()

    def second(k, d, hop):
        buf, major, minor, peer = streams[k][:4]
        ref = buf.at[major, (minor - d + R) % R, :, ring_cols(k)]
        return send(ref, sent.at[k, 2], p1r.at[kind(k, d + hop)], peer(hop))

    FURTHER = ((2, 1), (R - 2, -1), (2, 2))

    def piece_of(k, c):
        start = (streams[k][2] // chunk + c + (c // 2) * (5 - 2 * c)) % NC
        return pl.ds(start * chunk, chunk)

    def bulk(k, way, s, c):
        buf, major, _, _, peer = streams[k][:5]
        sign = SIGN[way]
        ref = buf.at[(major - sign * (s - 1) + R) % R, piece_of(k, c), :, ring_cols(k)]
        return send(ref, sent.at[k, 0], bkr.at[k, s - 1, c], peer(sign))

    def is_sent(way, s, c):
        return s < half or (s == half and (c < NC // 2) == (way == 0))

    def side_cols(k, p):
        side, middle = streams[k][5:]
        return pl.ds(pl.multiple_of(p * (side + middle), 128), side)

    def cross(k, j, c):
        buf, major = streams[k][:2]
        ref = buf.at[(major + j + R) % R, piece_of(k, c), :, side_cols(k, par)]
        step = 1 + (nfs - 2) * (c // (NC // 2))
        return send(ref, sent.at[k, 1], xr.at[k, j_abs(j)], {"fs": (fs + step) % nfs})

    def j_abs(j):
        return max(j, -j)

    def crossed(k, j):
        if j >= 0:
            ref = streams[k][0].at[pl.ds(0, 2 if 0 < j < half else 1), :, :, side_cols(k, 1 - par)]
            send(ref, sent.at[k, 1], xr.at[k, j], {"fs": (fs + 1) % nfs}).wait_recv()

    def own_piece(k, c):
        for way in (0, 1):
            bulk(k, way, 1, c).start()

    def forward(k, s, c):
        ways = [way for way in (0, 1) if is_sent(way, s, c)]
        ref = streams[k][0].at[0, pl.ds(0, len(ways) * chunk), :, ring_cols(k)]
        send(ref, sent.at[k, 0], bkr.at[k, s - 1, c], {"fs": (fs + 1) % nfs}).wait_recv()
        for way in ways:
            if is_sent(way, s + 1, c):
                bulk(k, way, s + 1, c).start()
            if k < 2 or s < half:
                cross(k, -SIGN[way] * s, c).start()

    def late(k):
        buf, major, _, _, peer = streams[k][:5]
        for way in (0, 1):
            sign = SIGN[way]
            for c in range(NC):
                if is_sent(way, half, c):
                    ref = buf.at[(major - sign * (half - 1) + R) % R, piece_of(k, c), :, side_cols(k, 1 - par)]
                    send(ref, sent.at[k, 1], xr.at[k, half], peer(sign)).start()

    barrier = pltpu.get_barrier_semaphore()
    peers = [{"tp": 1 - tp}]
    peers += [{"sp": (sp + d + R * R) % (R * R)} for d in (1, -1)]
    peers += [{"fs": (fs + d) % nfs} for d in (1, nfs - 1)]
    for d in range(1, R):
        peers += [along_y(d), along_z(d)]
    for peer in peers:
        pl.semaphore_signal(barrier, inc=1, device_id=peer, device_id_type=MESH)

    local = []

    def place(src, dst):
        copy = pltpu.make_async_copy(src, dst, loc_sem.at[len(local)])
        copy.start()
        local.append(copy)

    side = pl.multiple_of(par * (nq // 2), 128)
    place(wq.at[:, pl.ds(side, nq // 2)], zi.at[a, b, :, pl.ds(pl.multiple_of(par * (nq // 2 + 2 * nk), 128), nq // 2)])
    place(wk, zi.at[a, b, :, pl.ds(nq // 2, nk)])
    place(wv, zi.at[a, b, :, pl.ds(nq // 2 + nk, nk)])
    place(wp.at[:, ring_cols(1)], yi.at[b, a, :, ring_cols(1)])
    place(x_hbm, xb.at[pl.ds(mine, own)])
    place(gain_hbm, gain)
    place(wa.at[:, ring_cols(2)], zo.at[z, y, :, ring_cols(2)])
    place(wo.at[:, ring_cols(3)], yo.at[y, z, :, ring_cols(3)])
    place(sink_hbm, sink)
    place(pmix_hbm.at[pl.ds(tp * pmix.shape[0], pmix.shape[0])], pmix)
    place(pgain_hbm.at[:, pl.ds(pl.multiple_of(tp * npool, 128), npool)], pgain)

    with scope("barrier"):
        pl.semaphore_wait(barrier, len(peers))
        for copy in local[:4]:
            copy.wait()

    tokens = send(xb.at[pl.ds(mine, own)], tok_sem.at[0], tok_sem.at[1], {"tp": 1 - tp})
    def norm(start):
        def body(i, carry):
            r = pl.multiple_of(start + i * 32, 32)
            v = xb[pl.ds(r, 32), :].astype(F32)
            scale = lax.rsqrt(jnp.mean(v * v, axis=1, keepdims=True) + EPSILON)
            n = v * scale * gain[...]
            for j in range(R):
                nb[tp, j, pl.ds(r, 32), :] = n[:, j * block : (j + 1) * block].astype(BF16)
            lane = lax.broadcasted_iota(jnp.int32, (32, 128), 1) // SHARD
            for j in range(R):
                for g in range(block // 128):
                    t = None
                    for q in range(128 // SHARD):
                        at = (g * (128 // SHARD) + q) * block + j * SHARD
                        a = n[:, at // 128 * 128 : at // 128 * 128 + 128]
                        turn = (q * SHARD - at % 128) % 128
                        a = pltpu.roll(a, turn, 1) if turn else a
                        t = a if t is None else jnp.where(lane == q, a, t)
                    nb[1 - tp, j, pl.ds(r, 32), g * 128 : (g + 1) * 128] = t.astype(BF16)
            return carry

        lax.fori_loop(0, own // 32, body, 0)

    def zero(i, carry):
        r = pl.multiple_of(i * 32, 32)
        accz[pl.ds(r, 32), :] = jnp.zeros((32, accz.shape[1]), F32)
        accy[pl.ds(r, 32), :] = jnp.zeros((32, accy.shape[1]), F32)
        return carry

    def in_z(j):
        n = (a + j + R) % R
        with scope("in_z"):
            crossed(0, j)
            accz[...] += jnp.dot(nb[0, n], zi[n].reshape(block, zi.shape[3]), preferred_element_type=F32)

    def in_y(j):
        n = (b + j + R) % R
        with scope("in_y"):
            crossed(1, j)
            accy[...] += jnp.dot(nb[1, n], yi[n].reshape(block, yi.shape[3]), preferred_element_type=F32)

    for d in (half, 3, R - 3, 2, R - 2, 1, R - 1):
        first(0, d).start()
        first(1, d).start()
    for copy in local[4:]:
        copy.wait()
    tokens.start()
    with scope("norm"):
        lax.fori_loop(0, rows // 32, zero, 0)
        norm(mine)
    for k in (2, 3):
        for d in (1, R - 1, 2, R - 2):
            first(k, d).start()
    with scope("norm"):
        px[0:WIN, :] = jnp.zeros((WIN, npool), BF16)
        tokens.wait_recv()
        norm(theirs)
    with scope("first"):
        for c in INWARD:
            for k in (0, 1):
                minor = streams[k][2]
                start = (minor // chunk + c + (c // 2) * (5 - 2 * c)) % NC * chunk
                if c == 0:
                    first(k, (2 * (minor % 2) + R - 1) % R).wait_recv()
                else:
                    first(k, (minor - start + R) % R).wait_recv()
                    first(k, (minor - start - 1 + R) % R).wait_recv()
                own_piece(k, c)
                cross(k, 0, c).start()

    order = [0] + [j for s in range(1, half) for j in (s, -s)] + [half]
    ready = [lambda j=j, f=f: f(j) for j in order for f in (in_z, in_y)]
    steps = [(s, c) for s in range(1, half) for c in range(NC)]
    steps += [(half, c) for c in (0, 2, 1, 3)]
    in_steps = [(s, c) for s in range(1, half + 1) for c in INWARD]
    with scope("second"):
        for k in (2, 3):
            arrived(k, 1, 2)
            for d, hop in FURTHER:
                second(k, d, hop).start()
    for i, (s, c) in enumerate(in_steps):
        with scope("in_ring"):
            forward(0, s, c)
            forward(1, s, c)
        if i == 3 * NC - 1:
            with scope("own_out"):
                for k in (2, 3):
                    arrived(k, 0, R - 3)
                    for n in range(NC):
                        own_piece(k, n)
        for _ in range(4 if i == 3 * NC - 1 else i in (4, 5, 7, 8, 9, 10)):
            ready.pop(0)()
    for k in (2, 3):
        for c in range(NC):
            cross(k, 0, c).start()

    def split_z(i, carry):
        r = pl.multiple_of(i * 128, 128)
        e = pl.multiple_of(WIN + i * 128, 128)
        for p in range(heads // 2):
            at = p * 128 if p < heads // 4 else p * 128 + 2 * nk
            q = accz[pl.ds(r, 128), at : at + 128] * (HEAD ** (-0.5))
            qs[pl.ds(r, 128), p * 128 : (p + 1) * 128] = q.astype(BF16)
        for ref, at in ((kx, nq // 2), (vx, nq // 2 + nk)):
            t = accz[pl.ds(r, 128), at : at + nk]
            ref[0, pl.ds(e, 128), :] = t.astype(BF16)
            ref[1, pl.ds(e, 128), :] = pltpu.roll(t, HEAD, 1).astype(BF16)
        return carry

    def split_y(i, carry):
        r = pl.multiple_of(i * 32, 32)
        e = pl.multiple_of(WIN + i * 32, 32)
        px[pl.ds(e, 32), :] = accy[pl.ds(r, 32), :].astype(BF16)
        return carry

    def tail(i, ref, n):
        src, dst = pl.ds(WIN + rows - n, n), pl.ds(WIN - n, n)
        return pltpu.make_async_remote_copy(
            src_ref=ref.at[src] if i == 2 else ref.at[0, src],
            dst_ref=ref.at[dst] if i == 2 else ref.at[0, dst],
            send_sem=hls.at[i], recv_sem=hlr.at[i],
            device_id={"sp": (sp + 1) % (R * R)}, device_id_type=MESH,
        )

    tails = (tail(0, kx, WIN), tail(1, vx, WIN), tail(2, px, 16))

    def attend(b):
        r = pl.multiple_of(b * WIN, WIN)
        i = lax.broadcasted_iota(jnp.int32, (WIN, WIN), 0)
        j = lax.broadcasted_iota(jnp.int32, (WIN, 128), 1)
        older = j > i
        missing = jnp.where((sp == 0) & (b == 0), -jnp.inf, 0.0)
        left = j < HEAD
        halves = (jnp.where(left, 1.0, 0.0).astype(BF16), jnp.where(left, 0.0, 1.0).astype(BF16))
        logs = jnp.zeros((WIN, 128), F32)
        width = heads // 2
        for g in (0, 1):
            scores = []
            for h in range(g * width, (g + 1) * width):
                pair = qs[pl.ds(r, WIN), h // 2 * 128 : h // 2 * 128 + 128]
                score = lax.dot_general(
                    pair * halves[h % 2], kx[h % 2 ^ g, pl.ds(r, 2 * WIN), :], (((1,), (1,)), ((), ())),
                    preferred_element_type=F32,
                )
                scores.append(jnp.where(older, score[:, :WIN] + missing, score[:, WIN:]))
            sinks = [sink[tp * heads + g * width + n] for n in range(width)]
            tops = [jnp.maximum(jnp.max(v, axis=1, keepdims=True), s) for v, s in zip(scores, sinks)]
            weights = [jnp.exp(v - t) for v, t in zip(scores, tops)]
            totals = [jnp.sum(v, axis=1, keepdims=True) + jnp.exp(s - t) for v, s, t in zip(weights, sinks, tops)]
            outs = []
            for n in range(width):
                probs = weights[n] * (1.0 / totals[n])
                band = jnp.concatenate(
                    [jnp.where(older, probs, 0.0).astype(BF16), jnp.where(older, 0.0, probs).astype(BF16)], axis=1
                )
                outs.append(jnp.dot(band, vx[n % 2 ^ g, pl.ds(r, 2 * WIN), :], preferred_element_type=F32))
            for n in range(width):
                logs = jnp.where(j == g * width + n, tops[n] + jnp.log(totals[n]), logs)
            for n in range(0, width, 2):
                at = (g * width + n) // 2 * 128
                ma[pl.ds(r, WIN), at : at + 128] = jnp.where(left, outs[n], outs[n + 1]).astype(BF16)
        lse[:, pl.ds(r, WIN)] = jnp.transpose(logs)[:heads, :]

    def attend_at(b):
        with scope("attend"):
            attend(b)

    def pool(b):
        r = pl.multiple_of(b * WIN, WIN)
        i = lax.broadcasted_iota(jnp.int32, (WIN, 2 * WIN), 0)
        j = lax.broadcasted_iota(jnp.int32, (WIN, 2 * WIN), 1)
        low = jnp.where((sp == 0) & (b == 0), WIN, 0)
        lag = i + WIN - j
        pos = sp * rows + b * WIN + lax.broadcasted_iota(jnp.int32, (WIN, 1), 0)
        for g in range(npool // POOL_CH):
            cols = slice(g * POOL_CH, (g + 1) * POOL_CH)
            span = jnp.where(tp == 0, 2 << g, 8 << g)
            band = jnp.where((lag >= 0) & (lag < span) & (j >= low), 1.0, 0.0).astype(BF16)
            ext = px[pl.ds(r, 2 * WIN), cols]
            trailing = jnp.dot(band, ext, preferred_element_type=F32)
            count = jnp.minimum(pos + 1, span).astype(F32)
            centred = (trailing * (1.0 / count) - ext[WIN:].astype(F32)).astype(BF16)
            product = jnp.dot(centred, pmix[g], preferred_element_type=F32)
            mp[pl.ds(r, WIN), cols] = (product * pgain[:, cols]).astype(BF16)

    def pool_all(b, carry):
        pool(b)
        return carry

    def out_z(t, carry):
        for n in range(R // 2):
            @pl.when(t == n)
            def _():
                if n == 2:
                    for k in (2, 3):
                        crossed(k, half - 1)
                        late(k)
                for step in steps[2 * NC + 2 + max(n, 2 * n - 2) :][: 1 if n < 2 else 2]:
                    out_step(*step)
                if n != 2:
                    crossed(2, n + 1)

        for i in (2 * t, 2 * t + 1):
            n = (z + (i + 1) // 2 * (2 * (i % 2) - 1) + R) % R
            w = zo[n].reshape(block, zo.shape[3])
            ob[n] = lax.dot_general(ma[...], w, (((1,), (1,)), ((), ())), preferred_element_type=F32)
        return carry

    def split_all():
        with scope("split_z"):
            lax.fori_loop(0, rows // 128, split_z, 0)
            tails[0].start()
            tails[1].start()

    def split_pool():
        with scope("split_y"):
            lax.fori_loop(0, rows // 32, split_y, 0)
            tails[2].start()

    def pool_now():
        with scope("tail_wait"):
            for t in tails:
                t.wait_recv()
            for ref in (kx, vx):
                ref[1, 0:WIN, :] = pltpu.roll(ref[0, 0:WIN, :].astype(F32), HEAD, 1).astype(BF16)
        with scope("pool"):
            pool(0)

    def out_step(s, c):
        with scope("out_ring"):
            forward(2, s, c)
            forward(3, s, c)

    def attend_step(c, carry):
        attend_at(c + 1)
        for n, step in enumerate(((2, 2), (2, 3), (3, 0))):
            @pl.when(c == n)
            def _():
                out_step(*step)

        return carry

    def pool_first():
        with scope("pool"):
            lax.fori_loop(1, rows // WIN, pool_all, 0)

    last_z, last_y = ready[-2:]
    out_step(1, 0)
    for n, piece in enumerate(ready[:-2]):
        piece()
        if n % 2:
            out_step(1, 1 + n // 2)
    last_y()
    split_pool()
    out_step(1, 3)
    pool_first()
    out_step(2, 0)
    last_z()
    split_all()
    out_step(2, 1)
    lax.fori_loop(0, rows // WIN - 1, attend_step, 0)
    pool_now()
    out_step(3, 1)
    attend_at(0)
    with scope("out_z"):
        crossed(2, 0)
        lax.fori_loop(0, R // 2, out_z, 0)

    def exchange(n):
        return pltpu.make_async_remote_copy(
            src_ref=give_b.at[pl.ds(2 * n, 2)], dst_ref=rb.at[pl.ds(2 * n, 2)],
            send_sem=exs.at[0], recv_sem=exr.at[n],
            device_id={"tp": 1 - tp}, device_id_type=MESH,
        )

    def give(m, carry):
        for n in (2 * m, 2 * m + 1):
            w = yo[:, n].reshape(block, yo.shape[3])
            ob[n] += lax.dot_general(mp[...], w, (((1,), (1,)), ((), ())), preferred_element_type=F32)
            give_b[n] = ob[n, pl.ds(theirs, own), :].astype(BF16)
        exchange(m).start()
        return carry

    with scope("out_y_wait"):
        for j in (0, 1, 2, half):
            crossed(3, j)
    with scope("give"):
        lax.fori_loop(0, R // 2, give, 0)
    with scope("keep"):
        for n in range(R):
            if n % 2 == 0:
                exchange(n // 2).wait_recv()
            out[:, n * block : (n + 1) * block] = (ob[n, pl.ds(mine, own), :] + rb[n].astype(F32)).astype(BF16)

    with scope("drain"):
        tokens.wait_send()
        for t in tails:
            t.wait_send()
        for k in range(4):
            buf = streams[k][0]
            parts = (
                buf.at[pl.ds(0, R - 1), :, :, ring_cols(k)],
                buf.at[:, :, :, side_cols(k, par)],
                buf.at[0, pl.ds(0, R - 1), :, ring_cols(k)],
            )
            for i, ref in enumerate(parts):
                send(ref, sent.at[k, i], xr.at[k, 0], {"fs": (fs + 1) % nfs}).wait_send()
        pltpu.make_async_remote_copy(
            src_ref=give_b, dst_ref=rb, send_sem=exs.at[0], recv_sem=exr.at[0],
            device_id={"tp": 1 - tp}, device_id_type=MESH,
        ).wait_send()


def leave(result, logs, result_hbm, logs_hbm, sem):
    copies = []
    rows = result.shape[0] // 4
    for n in range(4):
        part = pl.ds(n * rows, rows)
        copies.append(pltpu.make_async_copy(result.at[part], result_hbm.at[part], sem.at[n]))
    copies.append(pltpu.make_async_copy(logs, logs_hbm, sem.at[4]))
    for copy in copies:
        copy.start()
    for copy in copies:
        copy.wait()


def local(
    tokens, norm_gain, query_weight, key_matrix, value_matrix, pool_in_weight,
    head_sink_logit, pool_mix, pool_gain, attn_out_weight, pool_out_weight,
):
    R = RING
    own, width = tokens.shape[1:]
    rows = 2 * own
    block = R * SHARD
    nq = query_weight.shape[1]
    nk = key_matrix.shape[1]
    npool = pool_in_weight.shape[1]
    heads = nq // HEAD
    groups = pool_mix.shape[0]
    vmem = pl.BlockSpec(memory_space=pltpu.VMEM)
    anywhere = pl.BlockSpec(memory_space=pl.ANY)
    dma = pltpu.SemaphoreType.DMA
    result, logs = pl.pallas_call(
        kernel,
        name="mixer",
        out_shape=(
            pltpu.VMEM((own, width), BF16),
            pltpu.VMEM((heads, rows), F32),
        ),
        in_specs=[anywhere] * 11,
        out_specs=(vmem, vmem),
        scratch_shapes=[
            pltpu.VMEM((R, R, SHARD, nq + 2 * nk), BF16),
            pltpu.VMEM((R, R, SHARD, npool), BF16),
            pltpu.VMEM((R, R, SHARD, attn_out_weight.shape[0]), BF16),
            pltpu.VMEM((R, R, SHARD, pool_out_weight.shape[0]), BF16),
            pltpu.VMEM((rows, width), BF16),
            pltpu.VMEM((2, R, rows, block), BF16),
            pltpu.VMEM((rows, nq + 2 * nk), F32),
            pltpu.VMEM((rows, npool), F32),
            pltpu.VMEM((rows, nq), BF16),
            pltpu.VMEM((2, WIN + rows, nk), BF16),
            pltpu.VMEM((2, WIN + rows, nk), BF16),
            pltpu.VMEM((WIN + rows, npool), BF16),
            pltpu.VMEM((rows, nq), BF16),
            pltpu.VMEM((rows, npool), BF16),
            pltpu.VMEM((R, rows, block), F32),
            pltpu.VMEM((R, own, block), BF16),
            pltpu.VMEM((R, own, block), BF16),
            pltpu.SMEM((2 * heads,), F32),
            pltpu.VMEM((1, width), F32),
            pltpu.VMEM((groups // 2, POOL_CH, POOL_CH), BF16),
            pltpu.VMEM((1, npool), F32),
            dma((11,)),
            dma((2,)),
            dma((4, 3)),
            dma((2 * R + 4,)),
            dma((4, R // 2, CHUNKS)),
            dma((4, R // 2 + 1)),
            dma((3,)),
            dma((3,)),
            dma((1,)),
            dma((R // 2,)),
        ],
        compiler_params=pltpu.CompilerParams(
            collective_id=0, has_side_effects=True, vmem_limit_bytes=56 * 1024 * 1024
        ),
    )(
        tokens[0],
        norm_gain[None],
        query_weight,
        key_matrix,
        value_matrix,
        pool_in_weight,
        head_sink_logit,
        pool_mix,
        pool_gain[None],
        attn_out_weight.T,
        pool_out_weight.T,
    )
    result, logs = pl.pallas_call(
        leave,
        name="leave",
        out_shape=(
            jax.ShapeDtypeStruct((own, width), BF16),
            jax.ShapeDtypeStruct((heads, rows), F32),
        ),
        in_specs=[vmem, vmem],
        out_specs=(anywhere, anywhere),
        scratch_shapes=[dma((5,))],
        compiler_params=pltpu.CompilerParams(vmem_limit_bytes=4 * 1024 * 1024),
    )(result, logs)
    return (result[None], logs[None])


def solution(mesh):
    in_specs = (
        P("fs", ("sp", "tp"), None),
        P(),
        P("sp", "tp"),
        P("sp", "tp"),
        P("sp", "tp"),
        P("sp", "tp"),
        P(),
        P(),
        P(),
        P("tp", "sp"),
        P("tp", "sp"),
    )
    out_specs = (P("fs", ("sp", "tp"), None), P("fs", "tp", "sp"))
    return jax.shard_map(local, mesh=mesh, in_specs=in_specs, out_specs=out_specs, check_vma=False)
```

```python
import jax
import jax.numpy as jnp
from jax import lax
from jax.experimental import pallas as pl
from jax.experimental.pallas import tpu as pltpu
from jax.sharding import PartitionSpec as P

RING = 8
CHUNKS = 4
SHARD = 32
HEAD = 64
WIN = 128
POOL_CH = 256
EPSILON = 1e-06
F32 = jnp.float32
BF16 = jnp.bfloat16
MESH = pl.DeviceIdType.MESH
SIGN = (1, -1)
WIDE = (3, 0)
INWARD = (3, 1, 2, 0)


def kernel(
    x_hbm, gain_hbm, wq, wk, wv, wp, sink_hbm, pmix_hbm, pgain_hbm, wa, wo,
    out, lse,
    zi, yi, zo, yo, xb, nb, accz, accy, qs, kx, vx, px, ma, mp, ob, give_b, rb, sink, gain, pmix, pgain,
    loc_sem, tok_sem, sent, p1r, bkr, xr, hls, hlr, exs, exr,
):
    R = RING
    NC = CHUNKS
    half = R // 2
    chunk = R // NC
    block = R * SHARD
    rows = xb.shape[0]
    own = rows // 2
    sp = lax.axis_index("sp")
    tp = lax.axis_index("tp")
    fs = lax.axis_index("fs")
    nfs = lax.axis_size("fs")
    par = fs % 2
    z, y = sp // R, sp % R
    mine = pl.multiple_of(tp * own, own)
    theirs = pl.multiple_of((1 - tp) * own, own)
    nq, nk, npool = wq.shape[1], wk.shape[1], wp.shape[1]
    heads = nq // HEAD
    scope = jax.named_scope

    def along_y(d):
        return {"sp": z * R + (y + d + R) % R}

    def along_z(d):
        return {"sp": ((z + d + R) % R) * R + y}

    a, b = z + tp * (y - z), y + tp * (z - y)
    stride_a, stride_b = R - tp * (R - 1), 1 + tp * (R - 1)

    def along_a(d):
        return {"sp": (a + d + R) % R * stride_a + b * stride_b}

    def along_b(d):
        return {"sp": a * stride_a + (b + d + R) % R * stride_b}

    streams = (
        (zi, a, b, along_b, along_a, nq // 2, 2 * nk),
        (yi, b, a, along_a, along_b, npool // 4, npool // 2),
        (zo, z, y, along_y, along_z, nq // 4, nq // 2),
        (yo, y, z, along_z, along_y, npool // 4, npool // 2),
    )

    def ring_cols(k):
        side, middle = streams[k][5:]
        return pl.ds(pl.multiple_of(par * side, 128), side + middle)

    def send(ref, send_sem, recv_sem, peer):
        return pltpu.make_async_remote_copy(
            src_ref=ref, dst_ref=ref, send_sem=send_sem, recv_sem=recv_sem,
            device_id=peer, device_id_type=MESH,
        )

    def first(k, d):
        buf, major, minor, peer = streams[k][:4]
        return send(buf.at[major, minor, :, ring_cols(k)], sent.at[k, 2], p1r.at[kind(k, d)], peer(d))

    def kind(k, d):
        return 2 * R + 2 * (k - 2) + int(d % R in (2, R - 2)) if k > 1 else k * R + d

    def arrived(k, which, n):
        ref = streams[k][0].at[0, pl.ds(0, n), :, ring_cols(k)]
        send(ref, sent.at[k, 2], p1r.at[2 * R + 2 * (k - 2) + which], {"fs": (fs + 1) % nfs}).wait_recv()

    def second(k, d, hop):
        buf, major, minor, peer = streams[k][:4]
        ref = buf.at[major, (minor - d + R) % R, :, ring_cols(k)]
        return send(ref, sent.at[k, 2], p1r.at[kind(k, d + hop)], peer(hop))

    FURTHER = ((2, 1), (R - 2, -1), (2, 2))

    def piece_of(k, c):
        start = (streams[k][2] // chunk + c + (c // 2) * (5 - 2 * c)) % NC
        return pl.ds(start * chunk, chunk)

    def bulk(k, way, s, c):
        buf, major, _, _, peer = streams[k][:5]
        sign = SIGN[way]
        ref = buf.at[(major - sign * (s - 1) + R) % R, piece_of(k, c), :, across_cols(k, c, par, False)]
        return send(ref, sent.at[k, 0], bkr.at[k, s - 1, c], peer(sign))

    def is_sent(way, s, c):
        return s < half or (s == half and (c < NC // 2) == (way == 0))

    def across_cols(k, c, p, own_side, mine=False):
        side, middle = streams[k][5:]
        more = side if k == 1 and c in WIDE and not mine else 0
        width = side + more if own_side else side + middle - more
        return pl.ds(pl.multiple_of(p * (2 * side + middle - width), 128), width)

    def side_cols(k, p):
        return across_cols(k, NC, p, True)

    def cross(k, j, c):
        buf, major = streams[k][:2]
        ref = buf.at[(major + j + R) % R, piece_of(k, c), :, across_cols(k, c, par, True, j == 0)]
        step = 1 + (nfs - 2) * (c // (NC // 2))
        return send(ref, sent.at[k, 3 if k == 1 and j == 0 else 1], xr.at[k, j_abs(j)], {"fs": (fs + step) % nfs})

    def j_abs(j):
        return max(j, -j)

    def crossed(k, j):
        if j >= 0:
            blocks = 2 if 0 < j < half else 1
            ref = streams[k][0].at[pl.ds(0, blocks), :, :, side_cols(k, 1 - par)]
            if k == 1 and j > 0:
                ref = streams[k][0].at[0, pl.ds(0, 3 * blocks)]
            send(ref, sent.at[k, 1], xr.at[k, j], {"fs": (fs + 1) % nfs}).wait_recv()

    def own_piece(k, c):
        for way in (0, 1):
            bulk(k, way, 1, c).start()

    def forward(k, s, c):
        ways = [way for way in (0, 1) if is_sent(way, s, c)]
        ref = streams[k][0].at[0, pl.ds(0, len(ways) * chunk), :, across_cols(k, c, par, False)]
        send(ref, sent.at[k, 0], bkr.at[k, s - 1, c], {"fs": (fs + 1) % nfs}).wait_recv()
        for way in ways:
            if is_sent(way, s + 1, c):
                bulk(k, way, s + 1, c).start()
            if k < 2 or s < half:
                cross(k, -SIGN[way] * s, c).start()

    def late(k):
        buf, major, _, _, peer = streams[k][:5]
        for way in (0, 1):
            sign = SIGN[way]
            for c in range(NC):
                if is_sent(way, half, c):
                    ref = buf.at[(major - sign * (half - 1) + R) % R, piece_of(k, c), :, side_cols(k, 1 - par)]
                    send(ref, sent.at[k, 1], xr.at[k, half], peer(sign)).start()

    barrier = pltpu.get_barrier_semaphore()
    peers = [{"tp": 1 - tp}]
    peers += [{"sp": (sp + d + R * R) % (R * R)} for d in (1, -1)]
    peers += [{"fs": (fs + d) % nfs} for d in (1, nfs - 1)]
    for d in range(1, R):
        peers += [along_y(d), along_z(d)]
    for peer in peers:
        pl.semaphore_signal(barrier, inc=1, device_id=peer, device_id_type=MESH)

    local = []

    def place(src, dst):
        copy = pltpu.make_async_copy(src, dst, loc_sem.at[len(local)])
        copy.start()
        local.append(copy)

    side = pl.multiple_of(par * (nq // 2), 128)
    place(wq.at[:, pl.ds(side, nq // 2)], zi.at[a, b, :, pl.ds(pl.multiple_of(par * (nq // 2 + 2 * nk), 128), nq // 2)])
    place(wk, zi.at[a, b, :, pl.ds(nq // 2, nk)])
    place(wv, zi.at[a, b, :, pl.ds(nq // 2 + nk, nk)])
    place(wp.at[:, ring_cols(1)], yi.at[b, a, :, ring_cols(1)])
    place(x_hbm, xb.at[pl.ds(mine, own)])
    place(gain_hbm, gain)
    place(wa.at[:, ring_cols(2)], zo.at[z, y, :, ring_cols(2)])
    place(wo.at[:, ring_cols(3)], yo.at[y, z, :, ring_cols(3)])
    place(sink_hbm, sink)
    place(pmix_hbm.at[pl.ds(tp * pmix.shape[0], pmix.shape[0])], pmix)
    place(pgain_hbm.at[:, pl.ds(pl.multiple_of(tp * npool, 128), npool)], pgain)

    with scope("barrier"):
        pl.semaphore_wait(barrier, len(peers))
        for copy in local[:4]:
            copy.wait()

    tokens = send(xb.at[pl.ds(mine, own)], tok_sem.at[0], tok_sem.at[1], {"tp": 1 - tp})
    def norm(start):
        def body(i, carry):
            r = pl.multiple_of(start + i * 32, 32)
            v = xb[pl.ds(r, 32), :].astype(F32)
            scale = lax.rsqrt(jnp.mean(v * v, axis=1, keepdims=True) + EPSILON)
            n = v * scale * gain[...]
            for j in range(R):
                nb[tp, j, pl.ds(r, 32), :] = n[:, j * block : (j + 1) * block].astype(BF16)
            lane = lax.broadcasted_iota(jnp.int32, (32, 128), 1) // SHARD
            for j in range(R):
                for g in range(block // 128):
                    t = None
                    for q in range(128 // SHARD):
                        at = (g * (128 // SHARD) + q) * block + j * SHARD
                        a = n[:, at // 128 * 128 : at // 128 * 128 + 128]
                        turn = (q * SHARD - at % 128) % 128
                        a = pltpu.roll(a, turn, 1) if turn else a
                        t = a if t is None else jnp.where(lane == q, a, t)
                    nb[1 - tp, j, pl.ds(r, 32), g * 128 : (g + 1) * 128] = t.astype(BF16)
            return carry

        lax.fori_loop(0, own // 32, body, 0)

    def zero(i, carry):
        r = pl.multiple_of(i * 32, 32)
        accz[pl.ds(r, 32), :] = jnp.zeros((32, accz.shape[1]), F32)
        accy[pl.ds(r, 32), :] = jnp.zeros((32, accy.shape[1]), F32)
        return carry

    def in_z(j):
        n = (a + j + R) % R
        with scope("in_z"):
            crossed(0, j)
            accz[...] += jnp.dot(nb[0, n], zi[n].reshape(block, zi.shape[3]), preferred_element_type=F32)

    def in_y(j):
        n = (b + j + R) % R
        with scope("in_y"):
            crossed(1, j)
            accy[...] += jnp.dot(nb[1, n], yi[n].reshape(block, yi.shape[3]), preferred_element_type=F32)

    for d in (half, 3, R - 3, 2, R - 2, 1, R - 1):
        first(0, d).start()
        first(1, d).start()
    for copy in local[4:]:
        copy.wait()
    tokens.start()
    with scope("norm"):
        lax.fori_loop(0, rows // 32, zero, 0)
        norm(mine)
    for k in (2, 3):
        for d in (1, R - 1, 2, R - 2):
            first(k, d).start()
    with scope("norm"):
        px[0:WIN, :] = jnp.zeros((WIN, npool), BF16)
        tokens.wait_recv()
        norm(theirs)
    with scope("first"):
        for c in INWARD:
            for k in (0, 1):
                minor = streams[k][2]
                start = (minor // chunk + c + (c // 2) * (5 - 2 * c)) % NC * chunk
                if c == 0:
                    first(k, (2 * (minor % 2) + R - 1) % R).wait_recv()
                else:
                    first(k, (minor - start + R) % R).wait_recv()
                    first(k, (minor - start - 1 + R) % R).wait_recv()
                own_piece(k, c)
                cross(k, 0, c).start()

    order = [0] + [j for s in range(1, half) for j in (s, -s)] + [half]
    ready = [lambda j=j, f=f: f(j) for j in order for f in (in_z, in_y)]
    steps = [(s, c) for s in range(1, half) for c in range(NC)]
    steps += [(half, c) for c in (0, 2, 1, 3)]
    in_steps = [(s, c) for s in range(1, half + 1) for c in INWARD]
    with scope("second"):
        for k in (2, 3):
            arrived(k, 1, 2)
            for d, hop in FURTHER:
                second(k, d, hop).start()
    for i, (s, c) in enumerate(in_steps):
        with scope("in_ring"):
            forward(0, s, c)
            forward(1, s, c)
        if i == 3 * NC - 1:
            with scope("own_out"):
                for k in (2, 3):
                    arrived(k, 0, R - 3)
                    for n in range(NC):
                        own_piece(k, n)
        for _ in range(4 if i == 3 * NC - 1 else i in (4, 5, 7, 8, 9, 10)):
            ready.pop(0)()
    for k in (2, 3):
        for c in range(NC):
            cross(k, 0, c).start()

    def split_z(i, carry):
        r = pl.multiple_of(i * 128, 128)
        e = pl.multiple_of(WIN + i * 128, 128)
        for p in range(heads // 2):
            at = p * 128 if p < heads // 4 else p * 128 + 2 * nk
            q = accz[pl.ds(r, 128), at : at + 128] * (HEAD ** (-0.5))
            qs[pl.ds(r, 128), p * 128 : (p + 1) * 128] = q.astype(BF16)
        for ref, at in ((kx, nq // 2), (vx, nq // 2 + nk)):
            t = accz[pl.ds(r, 128), at : at + nk]
            ref[0, pl.ds(e, 128), :] = t.astype(BF16)
            ref[1, pl.ds(e, 128), :] = pltpu.roll(t, HEAD, 1).astype(BF16)
        return carry

    def split_y(i, carry):
        r = pl.multiple_of(i * 32, 32)
        e = pl.multiple_of(WIN + i * 32, 32)
        px[pl.ds(e, 32), :] = accy[pl.ds(r, 32), :].astype(BF16)
        return carry

    def tail(i, ref, n):
        src, dst = pl.ds(WIN + rows - n, n), pl.ds(WIN - n, n)
        return pltpu.make_async_remote_copy(
            src_ref=ref.at[src] if i == 2 else ref.at[0, src],
            dst_ref=ref.at[dst] if i == 2 else ref.at[0, dst],
            send_sem=hls.at[i], recv_sem=hlr.at[i],
            device_id={"sp": (sp + 1) % (R * R)}, device_id_type=MESH,
        )

    tails = (tail(0, kx, WIN), tail(1, vx, WIN), tail(2, px, 16))

    def attend(b):
        r = pl.multiple_of(b * WIN, WIN)
        i = lax.broadcasted_iota(jnp.int32, (WIN, WIN), 0)
        j = lax.broadcasted_iota(jnp.int32, (WIN, 128), 1)
        older = j > i
        missing = jnp.where((sp == 0) & (b == 0), -jnp.inf, 0.0)
        left = j < HEAD
        halves = (jnp.where(left, 1.0, 0.0).astype(BF16), jnp.where(left, 0.0, 1.0).astype(BF16))
        logs = jnp.zeros((WIN, 128), F32)
        width = heads // 2
        for g in (0, 1):
            scores = []
            for h in range(g * width, (g + 1) * width):
                pair = qs[pl.ds(r, WIN), h // 2 * 128 : h // 2 * 128 + 128]
                score = lax.dot_general(
                    pair * halves[h % 2], kx[h % 2 ^ g, pl.ds(r, 2 * WIN), :], (((1,), (1,)), ((), ())),
                    preferred_element_type=F32,
                )
                scores.append(jnp.where(older, score[:, :WIN] + missing, score[:, WIN:]))
            sinks = [sink[tp * heads + g * width + n] for n in range(width)]
            tops = [jnp.maximum(jnp.max(v, axis=1, keepdims=True), s) for v, s in zip(scores, sinks)]
            weights = [jnp.exp(v - t) for v, t in zip(scores, tops)]
            totals = [jnp.sum(v, axis=1, keepdims=True) + jnp.exp(s - t) for v, s, t in zip(weights, sinks, tops)]
            outs = []
            for n in range(width):
                probs = weights[n] * (1.0 / totals[n])
                band = jnp.concatenate(
                    [jnp.where(older, probs, 0.0).astype(BF16), jnp.where(older, 0.0, probs).astype(BF16)], axis=1
                )
                outs.append(jnp.dot(band, vx[n % 2 ^ g, pl.ds(r, 2 * WIN), :], preferred_element_type=F32))
            for n in range(width):
                logs = jnp.where(j == g * width + n, tops[n] + jnp.log(totals[n]), logs)
            for n in range(0, width, 2):
                at = (g * width + n) // 2 * 128
                ma[pl.ds(r, WIN), at : at + 128] = jnp.where(left, outs[n], outs[n + 1]).astype(BF16)
        lse[:, pl.ds(r, WIN)] = jnp.transpose(logs)[:heads, :]

    def attend_at(b):
        with scope("attend"):
            attend(b)

    def pool(b):
        r = pl.multiple_of(b * WIN, WIN)
        i = lax.broadcasted_iota(jnp.int32, (WIN, 2 * WIN), 0)
        j = lax.broadcasted_iota(jnp.int32, (WIN, 2 * WIN), 1)
        low = jnp.where((sp == 0) & (b == 0), WIN, 0)
        lag = i + WIN - j
        pos = sp * rows + b * WIN + lax.broadcasted_iota(jnp.int32, (WIN, 1), 0)
        for g in range(npool // POOL_CH):
            cols = slice(g * POOL_CH, (g + 1) * POOL_CH)
            span = jnp.where(tp == 0, 2 << g, 8 << g)
            band = jnp.where((lag >= 0) & (lag < span) & (j >= low), 1.0, 0.0).astype(BF16)
            ext = px[pl.ds(r, 2 * WIN), cols]
            trailing = jnp.dot(band, ext, preferred_element_type=F32)
            count = jnp.minimum(pos + 1, span).astype(F32)
            centred = (trailing * (1.0 / count) - ext[WIN:].astype(F32)).astype(BF16)
            product = jnp.dot(centred, pmix[g], preferred_element_type=F32)
            mp[pl.ds(r, WIN), cols] = (product * pgain[:, cols]).astype(BF16)

    def pool_all(b, carry):
        pool(b)
        return carry

    def out_z(t, carry):
        for n in range(R // 2):
            @pl.when(t == n)
            def _():
                if n == 2:
                    for k in (2, 3):
                        crossed(k, half - 1)
                        late(k)
                for step in steps[2 * NC + 2 + max(n, 2 * n - 2) :][: 1 if n < 2 else 2]:
                    out_step(*step)
                if n != 2:
                    crossed(2, n + 1)

        for i in (2 * t, 2 * t + 1):
            n = (z + (i + 1) // 2 * (2 * (i % 2) - 1) + R) % R
            w = zo[n].reshape(block, zo.shape[3])
            ob[n] = lax.dot_general(ma[...], w, (((1,), (1,)), ((), ())), preferred_element_type=F32)
        return carry

    def split_all():
        with scope("split_z"):
            lax.fori_loop(0, rows // 128, split_z, 0)
            tails[0].start()
            tails[1].start()

    def split_pool():
        with scope("split_y"):
            lax.fori_loop(0, rows // 32, split_y, 0)
            tails[2].start()

    def pool_now():
        with scope("tail_wait"):
            for t in tails:
                t.wait_recv()
            for ref in (kx, vx):
                ref[1, 0:WIN, :] = pltpu.roll(ref[0, 0:WIN, :].astype(F32), HEAD, 1).astype(BF16)
        with scope("pool"):
            pool(0)

    def out_step(s, c):
        with scope("out_ring"):
            forward(2, s, c)
            forward(3, s, c)

    def attend_step(c, carry):
        attend_at(c + 1)
        for n, step in enumerate(((2, 2), (2, 3), (3, 0))):
            @pl.when(c == n)
            def _():
                out_step(*step)

        return carry

    def pool_first():
        with scope("pool"):
            lax.fori_loop(1, rows // WIN, pool_all, 0)

    last_z, last_y = ready[-2:]
    out_step(1, 0)
    for n, piece in enumerate(ready[:-2]):
        piece()
        if n % 2:
            out_step(1, 1 + n // 2)
    last_y()
    split_pool()
    out_step(1, 3)
    pool_first()
    out_step(2, 0)
    last_z()
    split_all()
    out_step(2, 1)
    lax.fori_loop(0, rows // WIN - 1, attend_step, 0)
    pool_now()
    out_step(3, 1)
    attend_at(0)
    with scope("out_z"):
        crossed(2, 0)
        lax.fori_loop(0, R // 2, out_z, 0)

    def exchange(n):
        return pltpu.make_async_remote_copy(
            src_ref=give_b.at[pl.ds(2 * n, 2)], dst_ref=rb.at[pl.ds(2 * n, 2)],
            send_sem=exs.at[0], recv_sem=exr.at[n],
            device_id={"tp": 1 - tp}, device_id_type=MESH,
        )

    def give(m, carry):
        for n in (2 * m, 2 * m + 1):
            w = yo[:, n].reshape(block, yo.shape[3])
            ob[n] += lax.dot_general(mp[...], w, (((1,), (1,)), ((), ())), preferred_element_type=F32)
            give_b[n] = ob[n, pl.ds(theirs, own), :].astype(BF16)
        exchange(m).start()
        return carry

    with scope("out_y_wait"):
        for j in (0, 1, 2, half):
            crossed(3, j)
    with scope("give"):
        lax.fori_loop(0, R // 2, give, 0)
    with scope("keep"):
        for n in range(R):
            if n % 2 == 0:
                exchange(n // 2).wait_recv()
            out[:, n * block : (n + 1) * block] = (ob[n, pl.ds(mine, own), :] + rb[n].astype(F32)).astype(BF16)

    with scope("drain"):
        tokens.wait_send()
        for t in tails:
            t.wait_send()
        for k in range(4):
            buf = streams[k][0]
            parts = (
                buf.at[pl.ds(0, R - 1), :, :, ring_cols(k)],
                buf.at[:, :, :, side_cols(k, par)],
                buf.at[0, pl.ds(0, R - 1), :, ring_cols(k)],
            )
            if k == 1:
                parts = (
                    buf.at[pl.ds(0, 5), pl.ds(0, R - 1)],
                    buf.at[pl.ds(0, 3), pl.ds(0, R - 1)],
                    parts[2],
                    buf.at[0, :, :, side_cols(k, par)],
                )
            for i, ref in enumerate(parts):
                send(ref, sent.at[k, i], xr.at[k, 0], {"fs": (fs + 1) % nfs}).wait_send()
        pltpu.make_async_remote_copy(
            src_ref=give_b, dst_ref=rb, send_sem=exs.at[0], recv_sem=exr.at[0],
            device_id={"tp": 1 - tp}, device_id_type=MESH,
        ).wait_send()


def leave(result, logs, result_hbm, logs_hbm, sem):
    copies = []
    rows = result.shape[0] // 4
    for n in range(4):
        part = pl.ds(n * rows, rows)
        copies.append(pltpu.make_async_copy(result.at[part], result_hbm.at[part], sem.at[n]))
    copies.append(pltpu.make_async_copy(logs, logs_hbm, sem.at[4]))
    for copy in copies:
        copy.start()
    for copy in copies:
        copy.wait()


def local(
    tokens, norm_gain, query_weight, key_matrix, value_matrix, pool_in_weight,
    head_sink_logit, pool_mix, pool_gain, attn_out_weight, pool_out_weight,
):
    R = RING
    own, width = tokens.shape[1:]
    rows = 2 * own
    block = R * SHARD
    nq = query_weight.shape[1]
    nk = key_matrix.shape[1]
    npool = pool_in_weight.shape[1]
    heads = nq // HEAD
    groups = pool_mix.shape[0]
    vmem = pl.BlockSpec(memory_space=pltpu.VMEM)
    anywhere = pl.BlockSpec(memory_space=pl.ANY)
    dma = pltpu.SemaphoreType.DMA
    result, logs = pl.pallas_call(
        kernel,
        name="mixer",
        out_shape=(
            pltpu.VMEM((own, width), BF16),
            pltpu.VMEM((heads, rows), F32),
        ),
        in_specs=[anywhere] * 11,
        out_specs=(vmem, vmem),
        scratch_shapes=[
            pltpu.VMEM((R, R, SHARD, nq + 2 * nk), BF16),
            pltpu.VMEM((R, R, SHARD, npool), BF16),
            pltpu.VMEM((R, R, SHARD, attn_out_weight.shape[0]), BF16),
            pltpu.VMEM((R, R, SHARD, pool_out_weight.shape[0]), BF16),
            pltpu.VMEM((rows, width), BF16),
            pltpu.VMEM((2, R, rows, block), BF16),
            pltpu.VMEM((rows, nq + 2 * nk), F32),
            pltpu.VMEM((rows, npool), F32),
            pltpu.VMEM((rows, nq), BF16),
            pltpu.VMEM((2, WIN + rows, nk), BF16),
            pltpu.VMEM((2, WIN + rows, nk), BF16),
            pltpu.VMEM((WIN + rows, npool), BF16),
            pltpu.VMEM((rows, nq), BF16),
            pltpu.VMEM((rows, npool), BF16),
            pltpu.VMEM((R, rows, block), F32),
            pltpu.VMEM((R, own, block), BF16),
            pltpu.VMEM((R, own, block), BF16),
            pltpu.SMEM((2 * heads,), F32),
            pltpu.VMEM((1, width), F32),
            pltpu.VMEM((groups // 2, POOL_CH, POOL_CH), BF16),
            pltpu.VMEM((1, npool), F32),
            dma((11,)),
            dma((2,)),
            dma((4, 4)),
            dma((2 * R + 4,)),
            dma((4, R // 2, CHUNKS)),
            dma((4, R // 2 + 1)),
            dma((3,)),
            dma((3,)),
            dma((1,)),
            dma((R // 2,)),
        ],
        compiler_params=pltpu.CompilerParams(
            collective_id=0, has_side_effects=True, vmem_limit_bytes=56 * 1024 * 1024
        ),
    )(
        tokens[0],
        norm_gain[None],
        query_weight,
        key_matrix,
        value_matrix,
        pool_in_weight,
        head_sink_logit,
        pool_mix,
        pool_gain[None],
        attn_out_weight.T,
        pool_out_weight.T,
    )
    result, logs = pl.pallas_call(
        leave,
        name="leave",
        out_shape=(
            jax.ShapeDtypeStruct((own, width), BF16),
            jax.ShapeDtypeStruct((heads, rows), F32),
        ),
        in_specs=[vmem, vmem],
        out_specs=(anywhere, anywhere),
        scratch_shapes=[dma((5,))],
        compiler_params=pltpu.CompilerParams(vmem_limit_bytes=4 * 1024 * 1024),
    )(result, logs)
    return (result[None], logs[None])


def solution(mesh):
    in_specs = (
        P("fs", ("sp", "tp"), None),
        P(),
        P("sp", "tp"),
        P("sp", "tp"),
        P("sp", "tp"),
        P("sp", "tp"),
        P(),
        P(),
        P(),
        P("tp", "sp"),
        P("tp", "sp"),
    )
    out_specs = (P("fs", ("sp", "tp"), None), P("fs", "tp", "sp"))
    return jax.shard_map(local, mesh=mesh, in_specs=in_specs, out_specs=out_specs, check_vma=False)
```

```python
import jax
import jax.numpy as jnp
from jax import lax
from jax.experimental import pallas as pl
from jax.experimental.pallas import tpu as pltpu
from jax.sharding import PartitionSpec as P

RING = 8
CHUNKS = 4
SHARD = 32
HEAD = 64
WIN = 128
POOL_CH = 256
EPSILON = 1e-06
F32 = jnp.float32
BF16 = jnp.bfloat16
MESH = pl.DeviceIdType.MESH
SIGN = (1, -1)
WIDE = (3, 0)
INWARD = (3, 1, 2, 0)


def kernel(
    x_hbm, gain_hbm, wq, wk, wv, wp, sink_hbm, pmix_hbm, pgain_hbm, wa, wo,
    out, lse,
    zi, yi, zo, yo, xb, nb, accz, accy, qs, kx, vx, px, ma, mp, ob, give_b, rb, sink, gain, pmix, pgain,
    loc_sem, tok_sem, sent, p1r, bkr, xr, hls, hlr, exs, exr,
):
    R = RING
    NC = CHUNKS
    half = R // 2
    chunk = R // NC
    block = R * SHARD
    rows = xb.shape[0]
    own = rows // 2
    sp = lax.axis_index("sp")
    tp = lax.axis_index("tp")
    fs = lax.axis_index("fs")
    nfs = lax.axis_size("fs")
    par = fs % 2
    z, y = sp // R, sp % R
    mine = pl.multiple_of(tp * own, own)
    theirs = pl.multiple_of((1 - tp) * own, own)
    nq, nk, npool = wq.shape[1], wk.shape[1], wp.shape[1]
    heads = nq // HEAD
    scope = jax.named_scope

    def along_y(d):
        return {"sp": z * R + (y + d + R) % R}

    def along_z(d):
        return {"sp": ((z + d + R) % R) * R + y}

    a, b = z + tp * (y - z), y + tp * (z - y)
    stride_a, stride_b = R - tp * (R - 1), 1 + tp * (R - 1)

    def along_a(d):
        return {"sp": (a + d + R) % R * stride_a + b * stride_b}

    def along_b(d):
        return {"sp": a * stride_a + (b + d + R) % R * stride_b}

    streams = (
        (zi, a, b, along_b, along_a, nq // 2, 2 * nk),
        (yi, b, a, along_a, along_b, npool // 4, npool // 2),
        (zo, z, y, along_y, along_z, nq // 4, nq // 2),
        (yo, y, z, along_z, along_y, npool // 4, npool // 2),
    )

    def ring_cols(k):
        side, middle = streams[k][5:]
        return pl.ds(pl.multiple_of(par * side, 128), side + middle)

    def send(ref, send_sem, recv_sem, peer):
        return pltpu.make_async_remote_copy(
            src_ref=ref, dst_ref=ref, send_sem=send_sem, recv_sem=recv_sem,
            device_id=peer, device_id_type=MESH,
        )

    def first(k, d):
        buf, major, minor, peer = streams[k][:4]
        return send(buf.at[major, minor, :, ring_cols(k)], sent.at[k, 2], p1r.at[kind(k, d)], peer(d))

    def kind(k, d):
        return 2 * R + 2 * (k - 2) + int(d % R in (2, R - 2)) if k > 1 else k * R + d

    def arrived(k, which, n):
        ref = streams[k][0].at[0, pl.ds(0, n), :, ring_cols(k)]
        send(ref, sent.at[k, 2], p1r.at[2 * R + 2 * (k - 2) + which], {"fs": (fs + 1) % nfs}).wait_recv()

    def second(k, d, hop):
        buf, major, minor, peer = streams[k][:4]
        ref = buf.at[major, (minor - d + R) % R, :, ring_cols(k)]
        return send(ref, sent.at[k, 2], p1r.at[kind(k, d + hop)], peer(hop))

    FURTHER = ((2, 1), (R - 2, -1), (2, 2))

    def piece_of(k, c):
        start = (streams[k][2] // chunk + c + (c // 2) * (5 - 2 * c)) % NC
        return pl.ds(start * chunk, chunk)

    def bulk(k, way, s, c):
        buf, major, _, _, peer = streams[k][:5]
        sign = SIGN[way]
        ref = buf.at[(major - sign * (s - 1) + R) % R, piece_of(k, c), :, across_cols(k, c, par, False)]
        return send(ref, sent.at[k, 0], bkr.at[min(k, 2), s - 1, c], peer(sign))

    def is_sent(way, s, c):
        return s < half or (s == half and (c < NC // 2) == (way == 0))

    def across_cols(k, c, p, own_side, mine=False):
        side, middle = streams[k][5:]
        more = side if k == 1 and c in WIDE and not mine else 0
        width = side + more if own_side else side + middle - more
        return pl.ds(pl.multiple_of(p * (2 * side + middle - width), 128), width)

    def side_cols(k, p):
        return across_cols(k, NC, p, True)

    def cross(k, j, c):
        buf, major = streams[k][:2]
        ref = buf.at[(major + j + R) % R, piece_of(k, c), :, across_cols(k, c, par, True, j == 0)]
        step = 1 + (nfs - 2) * (c // (NC // 2))
        return send(ref, sent.at[k, 3 if k == 1 and j == 0 else 1], xr.at[k, j_abs(j)], {"fs": (fs + step) % nfs})

    def j_abs(j):
        return max(j, -j)

    def crossed(k, j):
        if j >= 0:
            blocks = 2 if 0 < j < half else 1
            ref = streams[k][0].at[pl.ds(0, blocks), :, :, side_cols(k, 1 - par)]
            if k == 1 and j > 0:
                ref = streams[k][0].at[0, pl.ds(0, 3 * blocks)]
            send(ref, sent.at[k, 1], xr.at[k, j], {"fs": (fs + 1) % nfs}).wait_recv()

    def own_piece(k, c):
        for way in (0, 1):
            bulk(k, way, 1, c).start()

    def forward(k, s, c):
        ways = [way for way in (0, 1) if is_sent(way, s, c)]
        if k < 3:
            streams_waited = 1 if k < 2 else 2
            ref = streams[k][0].at[0, pl.ds(0, streams_waited * len(ways) * chunk), :, across_cols(k, c, par, False)]
            send(ref, sent.at[k, 0], bkr.at[k, s - 1, c], {"fs": (fs + 1) % nfs}).wait_recv()
        for way in ways:
            if is_sent(way, s + 1, c):
                bulk(k, way, s + 1, c).start()
            if k < 2 or s < half:
                cross(k, -SIGN[way] * s, c).start()

    def late(k):
        buf, major, _, _, peer = streams[k][:5]
        for way in (0, 1):
            sign = SIGN[way]
            for c in range(NC):
                if is_sent(way, half, c):
                    ref = buf.at[(major - sign * (half - 1) + R) % R, piece_of(k, c), :, side_cols(k, 1 - par)]
                    send(ref, sent.at[k, 1], xr.at[k, half], peer(sign)).start()

    barrier = pltpu.get_barrier_semaphore()
    peers = [{"tp": 1 - tp}]
    peers += [{"sp": (sp + d + R * R) % (R * R)} for d in (1, -1)]
    peers += [{"fs": (fs + d) % nfs} for d in (1, nfs - 1)]
    for d in range(1, R):
        peers += [along_y(d), along_z(d)]
    for peer in peers:
        pl.semaphore_signal(barrier, inc=1, device_id=peer, device_id_type=MESH)

    local = []

    def place(src, dst):
        copy = pltpu.make_async_copy(src, dst, loc_sem.at[len(local)])
        copy.start()
        local.append(copy)

    side = pl.multiple_of(par * (nq // 2), 128)
    place(wq.at[:, pl.ds(side, nq // 2)], zi.at[a, b, :, pl.ds(pl.multiple_of(par * (nq // 2 + 2 * nk), 128), nq // 2)])
    place(wk, zi.at[a, b, :, pl.ds(nq // 2, nk)])
    place(wv, zi.at[a, b, :, pl.ds(nq // 2 + nk, nk)])
    place(wp.at[:, ring_cols(1)], yi.at[b, a, :, ring_cols(1)])
    place(x_hbm, xb.at[pl.ds(mine, own)])
    place(gain_hbm, gain)
    place(wa.at[:, ring_cols(2)], zo.at[z, y, :, ring_cols(2)])
    place(wo.at[:, ring_cols(3)], yo.at[y, z, :, ring_cols(3)])
    place(sink_hbm, sink)
    place(pmix_hbm.at[pl.ds(tp * pmix.shape[0], pmix.shape[0])], pmix)
    place(pgain_hbm.at[:, pl.ds(pl.multiple_of(tp * npool, 128), npool)], pgain)

    with scope("barrier"):
        pl.semaphore_wait(barrier, len(peers))
        for copy in local[:4]:
            copy.wait()

    tokens = send(xb.at[pl.ds(mine, own)], tok_sem.at[0], tok_sem.at[1], {"tp": 1 - tp})
    def norm(start):
        def body(i, carry):
            r = pl.multiple_of(start + i * 32, 32)
            v = xb[pl.ds(r, 32), :].astype(F32)
            scale = lax.rsqrt(jnp.mean(v * v, axis=1, keepdims=True) + EPSILON)
            n = v * scale * gain[...]
            for j in range(R):
                nb[tp, j, pl.ds(r, 32), :] = n[:, j * block : (j + 1) * block].astype(BF16)
            lane = lax.broadcasted_iota(jnp.int32, (32, 128), 1) // SHARD
            for j in range(R):
                for g in range(block // 128):
                    t = None
                    for q in range(128 // SHARD):
                        at = (g * (128 // SHARD) + q) * block + j * SHARD
                        a = n[:, at // 128 * 128 : at // 128 * 128 + 128]
                        turn = (q * SHARD - at % 128) % 128
                        a = pltpu.roll(a, turn, 1) if turn else a
                        t = a if t is None else jnp.where(lane == q, a, t)
                    nb[1 - tp, j, pl.ds(r, 32), g * 128 : (g + 1) * 128] = t.astype(BF16)
            return carry

        lax.fori_loop(0, own // 32, body, 0)

    def zero(i, carry):
        r = pl.multiple_of(i * 32, 32)
        accz[pl.ds(r, 32), :] = jnp.zeros((32, accz.shape[1]), F32)
        accy[pl.ds(r, 32), :] = jnp.zeros((32, accy.shape[1]), F32)
        return carry

    def in_z(j):
        n = (a + j + R) % R
        with scope("in_z"):
            crossed(0, j)
            accz[...] += jnp.dot(nb[0, n], zi[n].reshape(block, zi.shape[3]), preferred_element_type=F32)

    def in_y(j):
        n = (b + j + R) % R
        with scope("in_y"):
            crossed(1, j)
            accy[...] += jnp.dot(nb[1, n], yi[n].reshape(block, yi.shape[3]), preferred_element_type=F32)

    for d in (half, 3, R - 3, 2, R - 2, 1, R - 1):
        first(0, d).start()
        first(1, d).start()
    for copy in local[4:]:
        copy.wait()
    tokens.start()
    with scope("norm"):
        lax.fori_loop(0, rows // 32, zero, 0)
        norm(mine)
    for k in (2, 3):
        for d in (1, R - 1, 2, R - 2):
            first(k, d).start()
    with scope("norm"):
        px[0:WIN, :] = jnp.zeros((WIN, npool), BF16)
        tokens.wait_recv()
        norm(theirs)
    with scope("first"):
        for c in INWARD:
            for k in (0, 1):
                minor = streams[k][2]
                start = (minor // chunk + c + (c // 2) * (5 - 2 * c)) % NC * chunk
                if c == 0:
                    first(k, (2 * (minor % 2) + R - 1) % R).wait_recv()
                else:
                    first(k, (minor - start + R) % R).wait_recv()
                    first(k, (minor - start - 1 + R) % R).wait_recv()
                own_piece(k, c)
                cross(k, 0, c).start()

    order = [0] + [j for s in range(1, half) for j in (s, -s)] + [half]
    ready = [lambda j=j, f=f: f(j) for j in order for f in (in_z, in_y)]
    steps = [(s, c) for s in range(1, half) for c in range(NC)]
    steps += [(half, c) for c in (0, 2, 1, 3)]
    in_steps = [(s, c) for s in range(1, half + 1) for c in INWARD]
    with scope("second"):
        for k in (2, 3):
            arrived(k, 1, 2)
            for d, hop in FURTHER:
                second(k, d, hop).start()
    for i, (s, c) in enumerate(in_steps):
        with scope("in_ring"):
            forward(0, s, c)
            forward(1, s, c)
        if i == 3 * NC - 1:
            with scope("own_out"):
                for k in (2, 3):
                    arrived(k, 0, R - 3)
                    for n in range(NC):
                        own_piece(k, n)
        for _ in range(4 if i == 3 * NC - 1 else i in (4, 5, 7, 8, 9, 10)):
            ready.pop(0)()
    for k in (2, 3):
        for c in range(NC):
            cross(k, 0, c).start()

    def split_z(i, carry):
        r = pl.multiple_of(i * 128, 128)
        e = pl.multiple_of(WIN + i * 128, 128)
        for p in range(heads // 2):
            at = p * 128 if p < heads // 4 else p * 128 + 2 * nk
            q = accz[pl.ds(r, 128), at : at + 128] * (HEAD ** (-0.5))
            qs[pl.ds(r, 128), p * 128 : (p + 1) * 128] = q.astype(BF16)
        for ref, at in ((kx, nq // 2), (vx, nq // 2 + nk)):
            t = accz[pl.ds(r, 128), at : at + nk]
            ref[0, pl.ds(e, 128), :] = t.astype(BF16)
            ref[1, pl.ds(e, 128), :] = pltpu.roll(t, HEAD, 1).astype(BF16)
        return carry

    def split_y(i, carry):
        r = pl.multiple_of(i * 32, 32)
        e = pl.multiple_of(WIN + i * 32, 32)
        px[pl.ds(e, 32), :] = accy[pl.ds(r, 32), :].astype(BF16)
        return carry

    def tail(i, ref, n):
        src, dst = pl.ds(WIN + rows - n, n), pl.ds(WIN - n, n)
        return pltpu.make_async_remote_copy(
            src_ref=ref.at[src] if i == 2 else ref.at[0, src],
            dst_ref=ref.at[dst] if i == 2 else ref.at[0, dst],
            send_sem=hls.at[i], recv_sem=hlr.at[i],
            device_id={"sp": (sp + 1) % (R * R)}, device_id_type=MESH,
        )

    tails = (tail(0, kx, WIN), tail(1, vx, WIN), tail(2, px, 16))

    def attend(b):
        r = pl.multiple_of(b * WIN, WIN)
        i = lax.broadcasted_iota(jnp.int32, (WIN, WIN), 0)
        j = lax.broadcasted_iota(jnp.int32, (WIN, 128), 1)
        older = j > i
        missing = jnp.where((sp == 0) & (b == 0), -jnp.inf, 0.0)
        left = j < HEAD
        halves = (jnp.where(left, 1.0, 0.0).astype(BF16), jnp.where(left, 0.0, 1.0).astype(BF16))
        logs = jnp.zeros((WIN, 128), F32)
        width = heads // 2
        for g in (0, 1):
            scores = []
            for h in range(g * width, (g + 1) * width):
                pair = qs[pl.ds(r, WIN), h // 2 * 128 : h // 2 * 128 + 128]
                score = lax.dot_general(
                    pair * halves[h % 2], kx[h % 2 ^ g, pl.ds(r, 2 * WIN), :], (((1,), (1,)), ((), ())),
                    preferred_element_type=F32,
                )
                scores.append(jnp.where(older, score[:, :WIN] + missing, score[:, WIN:]))
            sinks = [sink[tp * heads + g * width + n] for n in range(width)]
            tops = [jnp.maximum(jnp.max(v, axis=1, keepdims=True), s) for v, s in zip(scores, sinks)]
            weights = [jnp.exp(v - t) for v, t in zip(scores, tops)]
            totals = [jnp.sum(v, axis=1, keepdims=True) + jnp.exp(s - t) for v, s, t in zip(weights, sinks, tops)]
            outs = []
            for n in range(width):
                probs = weights[n] * (1.0 / totals[n])
                band = jnp.concatenate(
                    [jnp.where(older, probs, 0.0).astype(BF16), jnp.where(older, 0.0, probs).astype(BF16)], axis=1
                )
                outs.append(jnp.dot(band, vx[n % 2 ^ g, pl.ds(r, 2 * WIN), :], preferred_element_type=F32))
            for n in range(width):
                logs = jnp.where(j == g * width + n, tops[n] + jnp.log(totals[n]), logs)
            for n in range(0, width, 2):
                at = (g * width + n) // 2 * 128
                ma[pl.ds(r, WIN), at : at + 128] = jnp.where(left, outs[n], outs[n + 1]).astype(BF16)
        lse[:, pl.ds(r, WIN)] = jnp.transpose(logs)[:heads, :]

    def attend_at(b):
        with scope("attend"):
            attend(b)

    def pool(b):
        r = pl.multiple_of(b * WIN, WIN)
        i = lax.broadcasted_iota(jnp.int32, (WIN, 2 * WIN), 0)
        j = lax.broadcasted_iota(jnp.int32, (WIN, 2 * WIN), 1)
        low = jnp.where((sp == 0) & (b == 0), WIN, 0)
        lag = i + WIN - j
        pos = sp * rows + b * WIN + lax.broadcasted_iota(jnp.int32, (WIN, 1), 0)
        for g in range(npool // POOL_CH):
            cols = slice(g * POOL_CH, (g + 1) * POOL_CH)
            span = jnp.where(tp == 0, 2 << g, 8 << g)
            band = jnp.where((lag >= 0) & (lag < span) & (j >= low), 1.0, 0.0).astype(BF16)
            ext = px[pl.ds(r, 2 * WIN), cols]
            trailing = jnp.dot(band, ext, preferred_element_type=F32)
            count = jnp.minimum(pos + 1, span).astype(F32)
            centred = (trailing * (1.0 / count) - ext[WIN:].astype(F32)).astype(BF16)
            product = jnp.dot(centred, pmix[g], preferred_element_type=F32)
            mp[pl.ds(r, WIN), cols] = (product * pgain[:, cols]).astype(BF16)

    def pool_all(b, carry):
        pool(b)
        return carry

    def out_z(t, carry):
        for n in range(R // 2):
            @pl.when(t == n)
            def _():
                if n == 2:
                    for k in (2, 3):
                        crossed(k, half - 1)
                        late(k)
                for step in steps[2 * NC + 2 + max(n, 2 * n - 2) :][: 1 if n < 2 else 2]:
                    out_step(*step)
                if n != 2:
                    crossed(2, n + 1)

        for i in (2 * t, 2 * t + 1):
            n = (z + (i + 1) // 2 * (2 * (i % 2) - 1) + R) % R
            w = zo[n].reshape(block, zo.shape[3])
            ob[n] = lax.dot_general(ma[...], w, (((1,), (1,)), ((), ())), preferred_element_type=F32)
        return carry

    def split_all():
        with scope("split_z"):
            lax.fori_loop(0, rows // 128, split_z, 0)
            tails[0].start()
            tails[1].start()

    def split_pool():
        with scope("split_y"):
            lax.fori_loop(0, rows // 32, split_y, 0)
            tails[2].start()

    def pool_now():
        with scope("tail_wait"):
            for t in tails:
                t.wait_recv()
            for ref in (kx, vx):
                ref[1, 0:WIN, :] = pltpu.roll(ref[0, 0:WIN, :].astype(F32), HEAD, 1).astype(BF16)
        with scope("pool"):
            pool(0)

    def out_step(s, c):
        with scope("out_ring"):
            forward(2, s, c)
            forward(3, s, c)

    def attend_step(c, carry):
        attend_at(c + 1)
        for n, step in enumerate(((2, 2), (2, 3), (3, 0))):
            @pl.when(c == n)
            def _():
                out_step(*step)

        return carry

    def pool_first():
        with scope("pool"):
            lax.fori_loop(1, rows // WIN, pool_all, 0)

    last_z, last_y = ready[-2:]
    out_step(1, 0)
    for n, piece in enumerate(ready[:-2]):
        piece()
        if n % 2:
            out_step(1, 1 + n // 2)
    last_y()
    split_pool()
    out_step(1, 3)
    pool_first()
    out_step(2, 0)
    last_z()
    split_all()
    out_step(2, 1)
    lax.fori_loop(0, rows // WIN - 1, attend_step, 0)
    pool_now()
    out_step(3, 1)
    attend_at(0)
    with scope("out_z"):
        crossed(2, 0)
        lax.fori_loop(0, R // 2, out_z, 0)

    def exchange(n):
        return pltpu.make_async_remote_copy(
            src_ref=give_b.at[pl.ds(2 * n, 2)], dst_ref=rb.at[pl.ds(2 * n, 2)],
            send_sem=exs.at[0], recv_sem=exr.at[n],
            device_id={"tp": 1 - tp}, device_id_type=MESH,
        )

    def give(m, carry):
        for n in (2 * m, 2 * m + 1):
            w = yo[:, n].reshape(block, yo.shape[3])
            ob[n] += lax.dot_general(mp[...], w, (((1,), (1,)), ((), ())), preferred_element_type=F32)
            give_b[n] = ob[n, pl.ds(theirs, own), :].astype(BF16)
        exchange(m).start()
        return carry

    with scope("out_y_wait"):
        for j in (0, 1, 2, half):
            crossed(3, j)
    with scope("give"):
        lax.fori_loop(0, R // 2, give, 0)
    with scope("keep"):
        for n in range(R):
            if n % 2 == 0:
                exchange(n // 2).wait_recv()
            out[:, n * block : (n + 1) * block] = (ob[n, pl.ds(mine, own), :] + rb[n].astype(F32)).astype(BF16)

    with scope("drain"):
        tokens.wait_send()
        for t in tails:
            t.wait_send()
        for k in range(4):
            buf = streams[k][0]
            parts = (
                buf.at[pl.ds(0, R - 1), :, :, ring_cols(k)],
                buf.at[:, :, :, side_cols(k, par)],
                buf.at[0, pl.ds(0, R - 1), :, ring_cols(k)],
            )
            if k == 1:
                parts = (
                    buf.at[pl.ds(0, 5), pl.ds(0, R - 1)],
                    buf.at[pl.ds(0, 3), pl.ds(0, R - 1)],
                    parts[2],
                    buf.at[0, :, :, side_cols(k, par)],
                )
            for i, ref in enumerate(parts):
                send(ref, sent.at[k, i], xr.at[k, 0], {"fs": (fs + 1) % nfs}).wait_send()
        pltpu.make_async_remote_copy(
            src_ref=give_b, dst_ref=rb, send_sem=exs.at[0], recv_sem=exr.at[0],
            device_id={"tp": 1 - tp}, device_id_type=MESH,
        ).wait_send()


def leave(result, logs, result_hbm, logs_hbm, sem):
    copies = []
    rows = result.shape[0] // 4
    for n in range(4):
        part = pl.ds(n * rows, rows)
        copies.append(pltpu.make_async_copy(result.at[part], result_hbm.at[part], sem.at[n]))
    copies.append(pltpu.make_async_copy(logs, logs_hbm, sem.at[4]))
    for copy in copies:
        copy.start()
    for copy in copies:
        copy.wait()


def local(
    tokens, norm_gain, query_weight, key_matrix, value_matrix, pool_in_weight,
    head_sink_logit, pool_mix, pool_gain, attn_out_weight, pool_out_weight,
):
    R = RING
    own, width = tokens.shape[1:]
    rows = 2 * own
    block = R * SHARD
    nq = query_weight.shape[1]
    nk = key_matrix.shape[1]
    npool = pool_in_weight.shape[1]
    heads = nq // HEAD
    groups = pool_mix.shape[0]
    vmem = pl.BlockSpec(memory_space=pltpu.VMEM)
    anywhere = pl.BlockSpec(memory_space=pl.ANY)
    dma = pltpu.SemaphoreType.DMA
    result, logs = pl.pallas_call(
        kernel,
        name="mixer",
        out_shape=(
            pltpu.VMEM((own, width), BF16),
            pltpu.VMEM((heads, rows), F32),
        ),
        in_specs=[anywhere] * 11,
        out_specs=(vmem, vmem),
        scratch_shapes=[
            pltpu.VMEM((R, R, SHARD, nq + 2 * nk), BF16),
            pltpu.VMEM((R, R, SHARD, npool), BF16),
            pltpu.VMEM((R, R, SHARD, attn_out_weight.shape[0]), BF16),
            pltpu.VMEM((R, R, SHARD, pool_out_weight.shape[0]), BF16),
            pltpu.VMEM((rows, width), BF16),
            pltpu.VMEM((2, R, rows, block), BF16),
            pltpu.VMEM((rows, nq + 2 * nk), F32),
            pltpu.VMEM((rows, npool), F32),
            pltpu.VMEM((rows, nq), BF16),
            pltpu.VMEM((2, WIN + rows, nk), BF16),
            pltpu.VMEM((2, WIN + rows, nk), BF16),
            pltpu.VMEM((WIN + rows, npool), BF16),
            pltpu.VMEM((rows, nq), BF16),
            pltpu.VMEM((rows, npool), BF16),
            pltpu.VMEM((R, rows, block), F32),
            pltpu.VMEM((R, own, block), BF16),
            pltpu.VMEM((R, own, block), BF16),
            pltpu.SMEM((2 * heads,), F32),
            pltpu.VMEM((1, width), F32),
            pltpu.VMEM((groups // 2, POOL_CH, POOL_CH), BF16),
            pltpu.VMEM((1, npool), F32),
            dma((11,)),
            dma((2,)),
            dma((4, 4)),
            dma((2 * R + 4,)),
            dma((3, R // 2, CHUNKS)),
            dma((4, R // 2 + 1)),
            dma((3,)),
            dma((3,)),
            dma((1,)),
            dma((R // 2,)),
        ],
        compiler_params=pltpu.CompilerParams(
            collective_id=0, has_side_effects=True, vmem_limit_bytes=56 * 1024 * 1024
        ),
    )(
        tokens[0],
        norm_gain[None],
        query_weight,
        key_matrix,
        value_matrix,
        pool_in_weight,
        head_sink_logit,
        pool_mix,
        pool_gain[None],
        attn_out_weight.T,
        pool_out_weight.T,
    )
    result, logs = pl.pallas_call(
        leave,
        name="leave",
        out_shape=(
            jax.ShapeDtypeStruct((own, width), BF16),
            jax.ShapeDtypeStruct((heads, rows), F32),
        ),
        in_specs=[vmem, vmem],
        out_specs=(anywhere, anywhere),
        scratch_shapes=[dma((5,))],
        compiler_params=pltpu.CompilerParams(vmem_limit_bytes=4 * 1024 * 1024),
    )(result, logs)
    return (result[None], logs[None])


def solution(mesh):
    in_specs = (
        P("fs", ("sp", "tp"), None),
        P(),
        P("sp", "tp"),
        P("sp", "tp"),
        P("sp", "tp"),
        P("sp", "tp"),
        P(),
        P(),
        P(),
        P("tp", "sp"),
        P("tp", "sp"),
    )
    out_specs = (P("fs", ("sp", "tp"), None), P("fs", "tp", "sp"))
    return jax.shard_map(local, mesh=mesh, in_specs=in_specs, out_specs=out_specs, check_vma=False)
```
